512 devices in a mesh: sp: 64 (over z, y), tp: 8 (over x, core).
Axes of the slice: x: 4, y: 4, z: 16, core: 2. Of those that a mesh axis runs over, the one named last changes fastest.
Arguments:
- residual: bfloat16 [8192, 2048], P(('sp', 'tp')), may hold values from -24 to 24
- query_small: bfloat16 [8192, 768], P('sp', 'tp'), may hold values from -64 to 64
- query_large: bfloat16 [8192, 1280], P('sp', 'tp'), may hold values from -64 to 64
- latent: bfloat16 [8192, 256], P('sp'), may hold values from -6 to 6
- rope_key: bfloat16 [8192, 32], P('sp'), may hold values from -48 to 48
- key_up_small: bfloat16 [256, 512], P(None, 'tp'), may hold values from -0.375 to 0.375
- value_up_small: bfloat16 [256, 512], P(None, 'tp'), may hold values from -0.375 to 0.375
- key_up_large: bfloat16 [256, 1024], P(None, 'tp'), may hold values from -0.375 to 0.375
- value_up_large: bfloat16 [256, 1024], P(None, 'tp'), may hold values from -0.375 to 0.375
- out_small: bfloat16 [512, 2048], P('tp'), may hold values from -0.625 to 0.625
- out_large: bfloat16 [1024, 2048], P('tp'), may hold values from -0.625 to 0.625
- norm_gain: bfloat16 [2048], replicated, may hold values from 0.099609375 to 1.8984375
- gate_weight: bfloat16 [2048, 5632], P('sp', 'tp'), may hold values from -0.125 to 0.125
- up_weight: bfloat16 [2048, 5632], P('sp', 'tp'), may hold values from -0.125 to 0.125
- down_weight: bfloat16 [2048, 5632], P('sp', 'tp'), may hold values from -0.21875 to 0.21875
Outputs:
- layer_out: bfloat16 [8192, 2048], P(('sp', 'tp'))
The draws below stay inside these ranges and needn't reach their ends.
All inputs are finite; a program needn't handle non-finite values.
Results may differ from the reference program's by a relative error of at most 0.017.
Values may be sent and summed in bfloat16 or wider, within the bound.
No kernel may reach another device: no remote copies, remote signals or barrier semaphores. Data moves between devices by JAX's collectives and lax.ppermute only.
A program may use at most 64 MiB of HBM per device.

```python
import jax
import jax.numpy as jnp
from jax import lax

D = 2048
FF = 5632
HEADS_SMALL = 8
HEADS_LARGE = 8
HEAD_SMALL = 64
HEAD_LARGE = 128
ROPE = 32
LATENT = 256
TOKENS = 8192


def draw_residual(key, part):
    subkeys = jax.random.split(key, 3)
    lowest = 0.3
    highest = 3.0
    column = jnp.exp(jax.random.uniform(subkeys[0], (1, D), jnp.float32, jnp.log(lowest), jnp.log(highest)))
    rowscale = jnp.exp(jax.random.uniform(subkeys[1], (TOKENS, 1), jnp.float32, jnp.log(0.5), jnp.log(2.0)))
    sample = jnp.clip(jax.random.normal(subkeys[2], (TOKENS, D), jnp.float32), -4.0, 4.0)
    return jnp.clip(sample * rowscale * column, -24.0, 24.0).astype(jnp.bfloat16)


def drawn_query(key, head_count, head_size):
    span_width = head_size + ROPE
    sample = jnp.clip(2.5 * jax.random.normal(key, (TOKENS, head_count, span_width), jnp.float32), -10.0, 10.0)
    return sample.reshape(TOKENS, head_count * span_width).astype(jnp.bfloat16)


def draw_query_small(key, part):
    return drawn_query(jax.random.fold_in(key, 11), HEADS_SMALL, HEAD_SMALL)


def draw_query_large(key, part):
    return drawn_query(jax.random.fold_in(key, 23), HEADS_LARGE, HEAD_LARGE)


def draw_rope_key(key, part):
    sample = jnp.clip(jax.random.normal(key, (TOKENS, ROPE), jnp.float32), -6.0, 6.0)
    return sample.astype(jnp.bfloat16)


def steps_of(rng, dims, cuts, least, largest):
    def one(position, blocks):
        steps = jax.random.uniform(jax.random.fold_in(jax.random.fold_in(rng, 6), position), (blocks,), jnp.float32, least / len(cuts), largest / len(cuts))
        return jnp.repeat(jnp.exp(steps), dims[position] // blocks).reshape((-1,) + (1,) * (len(dims) - position - 1))

    loudness = one(*cuts[0])
    for cut in cuts[1:]:
        loudness = loudness * one(*cut)
    return loudness


def bell_draw(own_key, shape, spread, reach, shards=(), kind=jnp.bfloat16):
    gain = steps_of(own_key, shape, shards, -0.22, 0.18) if shards else 1.0
    drawn = jax.random.normal(own_key, shape, jnp.float32) * spread * gain
    return jnp.minimum(jnp.maximum(drawn, -reach), reach).astype(kind)


def setup_inputs(seed: int = 0) -> dict:
    seeds = jax.random.split(jax.random.key(seed), 16)
    residual = draw_residual(jax.random.fold_in(seeds[15], 71), 0)
    query_small = draw_query_small(jax.random.fold_in(seeds[15], 71), 0)
    query_large = draw_query_large(jax.random.fold_in(seeds[15], 71), 0)
    latent = bell_draw(seeds[3], (TOKENS, LATENT), 1.0, 6.0, ((0, 64),))
    rope_key = draw_rope_key(jax.random.fold_in(seeds[15], 71), 0)
    key_up_small = bell_draw(seeds[5], (LATENT, HEADS_SMALL * HEAD_SMALL), LATENT ** -0.5, 0.375, ((1, 8),))
    value_up_small = bell_draw(seeds[6], (LATENT, HEADS_SMALL * HEAD_SMALL), LATENT ** -0.5, 0.375, ((1, 8),))
    key_up_large = bell_draw(seeds[7], (LATENT, HEADS_LARGE * HEAD_LARGE), LATENT ** -0.5, 0.375, ((1, 8),))
    value_up_large = bell_draw(seeds[8], (LATENT, HEADS_LARGE * HEAD_LARGE), LATENT ** -0.5, 0.375, ((1, 8),))
    out_small = bell_draw(seeds[9], (HEADS_SMALL * HEAD_SMALL, D), ((HEADS_SMALL * HEAD_SMALL + HEADS_LARGE * HEAD_LARGE) // 16) ** -0.5, 0.625, ((0, 8),))
    out_large = bell_draw(seeds[10], (HEADS_LARGE * HEAD_LARGE, D), ((HEADS_SMALL * HEAD_SMALL + HEADS_LARGE * HEAD_LARGE) // 16) ** -0.5, 0.625, ((0, 8),))
    norm_gain = jnp.clip(1.0 + 0.18 * jax.random.normal(seeds[11], (D,), jnp.float32), 0.099609375, 1.8984375).astype(jnp.bfloat16)
    gate_weight = bell_draw(seeds[12], (D, FF), D ** -0.5, 0.125, ((0, 64), (1, 8)))
    up_weight = bell_draw(seeds[13], (D, FF), D ** -0.5, 0.125, ((0, 64), (1, 8)))
    down_weight = bell_draw(seeds[14], (D, FF), (FF // 8) ** -0.5, 0.21875, ((0, 64), (1, 8)))
    return {"residual": residual, "query_small": query_small, "query_large": query_large, "latent": latent, "rope_key": rope_key, "key_up_small": key_up_small, "value_up_small": value_up_small, "key_up_large": key_up_large, "value_up_large": value_up_large, "out_small": out_small, "out_large": out_large, "norm_gain": norm_gain, "gate_weight": gate_weight, "up_weight": up_weight, "down_weight": down_weight}


big_negative = -1e+30
rope_base = 500000.0
norm_eps = 1e-06

def stored(tensor):
    return lax.optimization_barrier(tensor.astype(jnp.bfloat16))

def rotate_stored(vectors, positions):
    span_width = vectors.shape[-1]
    half_width = span_width // 2
    inverse = 1.0 / rope_base ** (jnp.arange(0, span_width, 2, dtype=jnp.float32) / span_width)
    angles = positions.astype(jnp.float32)[:, None] * inverse[None, :]
    angle_shape = (vectors.shape[0],) + (1,) * (vectors.ndim - 2) + (half_width,)
    cosine = jnp.cos(angles).reshape(angle_shape)
    sine_table = jnp.sin(angles).reshape(angle_shape)
    leading = vectors[..., :half_width].astype(jnp.float32)
    trailing = vectors[..., half_width:].astype(jnp.float32)
    turned = jnp.concatenate([leading * cosine - trailing * sine_table, trailing * cosine + leading * sine_table], axis=-1)
    return stored(turned)

def attend_group(query, latent, key_up, value_up, turned_key, positions, head_count, head_size):
    shaped = query.reshape(TOKENS, head_count, head_size + ROPE)
    nope_part = shaped[..., :head_size]
    turned_query = rotate_stored(shaped[..., head_size:], positions)
    key_rows = stored(jnp.dot(latent, key_up, preferred_element_type=jnp.float32)).reshape(TOKENS, head_count, head_size)
    value_rows = stored(jnp.dot(latent, value_up, preferred_element_type=jnp.float32)).reshape(TOKENS, head_count, head_size)
    scale = (head_size + ROPE) ** (-0.5)
    block_rows = min(256, TOKENS)

    def one_block(block_index):
        offset = block_index * block_rows
        query_nope = lax.dynamic_slice_in_dim(nope_part, offset, block_rows, 0).astype(jnp.float32)
        query_turn = lax.dynamic_slice_in_dim(turned_query, offset, block_rows, 0).astype(jnp.float32)
        query_pos = offset + jnp.arange(block_rows, dtype=jnp.int32)
        scores = jnp.einsum('qhe,khe->qhk', query_nope, key_rows.astype(jnp.float32))
        scores = scores + jnp.einsum('qhr,kr->qhk', query_turn, turned_key.astype(jnp.float32))
        scores = scores * scale
        visible = positions[None, None, :] <= query_pos[:, None, None]
        masked = jnp.where(visible, scores, big_negative)
        maxima = lax.optimization_barrier(jnp.max(masked, axis=2, keepdims=True))
        weights = jnp.where(visible, jnp.exp(masked - maxima), 0.0)
        totals = lax.optimization_barrier(jnp.sum(weights, axis=2))
        rounded = stored(weights).astype(jnp.float32)
        result = jnp.einsum('qhk,khe->qhe', rounded, value_rows.astype(jnp.float32)) / totals[:, :, None]
        return result.reshape(block_rows, head_count * head_size).astype(jnp.bfloat16)
    blocks = lax.map(one_block, jnp.arange(TOKENS // block_rows, dtype=jnp.int32))
    return blocks.reshape(TOKENS, head_count * head_size)

def reference(residual, query_small, query_large, latent, rope_key, key_up_small, value_up_small, key_up_large, value_up_large, out_small, out_large, norm_gain, gate_weight, up_weight, down_weight):
    positions = jnp.arange(TOKENS, dtype=jnp.int32)
    turned_key = rotate_stored(rope_key, positions)
    attended_small = attend_group(query_small, latent, key_up_small, value_up_small, turned_key, positions, HEADS_SMALL, HEAD_SMALL)
    attended_large = attend_group(query_large, latent, key_up_large, value_up_large, turned_key, positions, HEADS_LARGE, HEAD_LARGE)
    mixed = jnp.dot(attended_small, out_small, preferred_element_type=jnp.float32)
    mixed = mixed + jnp.dot(attended_large, out_large, preferred_element_type=jnp.float32)
    mixed = stored(mixed)
    stream = stored(residual.astype(jnp.float32) + mixed.astype(jnp.float32))
    as_float = stream.astype(jnp.float32)
    normed = as_float * lax.rsqrt(lax.optimization_barrier(jnp.mean(as_float * as_float, axis=-1, keepdims=True)) + norm_eps)
    normed = (normed * norm_gain.astype(jnp.float32)[None, :]).astype(jnp.bfloat16)
    gate = jnp.dot(normed, gate_weight, preferred_element_type=jnp.float32)
    up_part = jnp.dot(normed, up_weight, preferred_element_type=jnp.float32)
    hidden = (jax.nn.silu(gate) * up_part).astype(jnp.bfloat16)
    channel = lax.dot_general(hidden, down_weight, (((1,), (1,)), ((), ())), preferred_element_type=jnp.float32)
    channel = stored(channel)
    return (as_float + 0.5 * channel.astype(jnp.float32)).astype(jnp.bfloat16)
```

```python
import jax
import jax.numpy as jnp
from jax import lax
from jax.experimental import pallas as pl
from jax.experimental.pallas import tpu as pltpu
from jax.sharding import Mesh
from jax.sharding import PartitionSpec as P

HEAD_SMALL = 64
HEAD_LARGE = 128
ROPE = 32
SCALE_SMALL = (HEAD_SMALL + ROPE) ** (-0.5)
SCALE_LARGE = (HEAD_LARGE + ROPE) ** (-0.5)

big_negative = -1e30
rope_base = 500000.0
norm_eps = 1e-06

NT = (((1,), (1,)), ((), ()))


def rotate(vectors, positions):
    span_width = vectors.shape[-1]
    half_width = span_width // 2
    inverse = 1.0 / rope_base ** (jnp.arange(0, span_width, 2, dtype=jnp.float32) / span_width)
    angles = positions.astype(jnp.float32)[:, None] * inverse[None, :]
    cosine = jnp.cos(angles)
    sine = jnp.sin(angles)
    leading = vectors[..., :half_width].astype(jnp.float32)
    trailing = vectors[..., half_width:].astype(jnp.float32)
    turned = jnp.concatenate(
        [leading * cosine - trailing * sine, trailing * cosine + leading * sine], axis=-1
    )
    return turned.astype(jnp.bfloat16)


def from_everyone(shard, axis):
    copies = jnp.broadcast_to(shard, (lax.axis_size(axis), *shard.shape))
    return lax.all_to_all(copies, axis, split_axis=0, concat_axis=0, tiled=True)


def exchanged(chunks, axis):
    return lax.all_to_all(chunks, axis, split_axis=0, concat_axis=0, tiled=True)


def partner(x):
    return lax.ppermute(x, "c", [(0, 1), (1, 0)])


def three_parts(v):
    high = v.astype(jnp.bfloat16).astype(jnp.float32)
    rest = v - high
    middle = rest.astype(jnp.bfloat16).astype(jnp.float32)
    low = (rest - middle).astype(jnp.bfloat16).astype(jnp.float32)
    return [high, middle, low]


def attention_kernel(
    place, query, mine, other, key_up_s, key_up_l, value_up_s, value_up_l, out, keys, turned
):
    z = place[0]
    y = place[1]
    c = place[2]
    n_x, n_z = mine.shape[0], mine.shape[1]
    for x in range(n_x):
        for k in range(n_z):
            lanes = pl.ds(128 * k, 128)
            here = pl.multiple_of(64 * x + 32 * c, 32)
            there = pl.multiple_of(64 * x + 32 * (1 - c), 32)
            keys[pl.ds(here, 32), lanes] = mine[x, k, 0:32, :]
            keys[pl.ds(there, 32), lanes] = other[x, k, 0:32, :]
    for k in range(n_z):
        rows = [mine[x, k, 32:40, :].astype(jnp.float32) for x in range(n_x)]
        turned[:, pl.ds(128 * k, 128)] = jnp.concatenate(rows, axis=0).astype(jnp.bfloat16)
    n_keys = 128 * n_z
    n_y = query.shape[0] // 128
    column = lax.broadcasted_iota(jnp.int32, (1, n_keys), 1)
    key_pos = (column // 128) * (128 * n_y) + y * 128 + column % 128
    key_up_small = key_up_s[...]
    key_up_large = key_up_l[...]
    value_up_small = value_up_s[...]
    value_up_large = value_up_l[...]
    lane = lax.broadcasted_iota(jnp.int32, (128, 64), 1)

    def head(nope, rope, key_up, value_up, scale, visible):
        wide = lax.dot_general(nope, key_up, NT, preferred_element_type=jnp.float32)
        score = jnp.dot(
            wide.astype(jnp.bfloat16), keys[...], preferred_element_type=jnp.float32
        ) + jnp.dot(rope, turned[...], preferred_element_type=jnp.float32)
        score = jnp.where(visible, score * scale, big_negative)
        top = jnp.max(score, axis=1, keepdims=True)
        weight = jnp.exp(score - top)
        total = jnp.sum(weight, axis=1, keepdims=True)
        summed = lax.dot_general(
            weight.astype(jnp.bfloat16), keys[...], NT, preferred_element_type=jnp.float32
        )
        summed = (summed / total).astype(jnp.bfloat16)
        value = jnp.dot(summed, value_up, preferred_element_type=jnp.float32)
        return value, top, total

    for j in range(n_y):
        rows = pl.ds(128 * j, 128)
        row = lax.broadcasted_iota(jnp.int32, (128, 1), 0)
        visible = key_pos <= z * (128 * n_y) + j * 128 + row
        q = query[rows, :]
        value_l, top_l, total_l = head(
            q[:, 0:128], q[:, 224:256], key_up_large, value_up_large, SCALE_LARGE, visible
        )
        value_s, top_s, total_s = head(
            q[:, 128:192], q[:, 192:224], key_up_small, value_up_small, SCALE_SMALL, visible
        )
        stats = jnp.zeros((128, 64), jnp.float32)
        parts = three_parts(top_l) + three_parts(total_l) + three_parts(top_s) + three_parts(total_s)
        for i, part in enumerate(parts):
            stats = jnp.where(lane == i, part, stats)
        out[rows, 0:128] = value_l.astype(jnp.bfloat16)
        out[rows, 128:256] = jnp.concatenate([value_s, stats], axis=1).astype(jnp.bfloat16)


def attention(place, query, mine, other, key_up_s, key_up_l, value_up_s, value_up_l):
    n_keys = 128 * mine.shape[1]
    vmem = pl.BlockSpec(memory_space=pltpu.VMEM)
    return pl.pallas_call(
        attention_kernel,
        out_shape=jax.ShapeDtypeStruct(query.shape, jnp.bfloat16),
        in_specs=[pl.BlockSpec(memory_space=pltpu.SMEM)] + [vmem] * 7,
        out_specs=vmem,
        scratch_shapes=[
            pltpu.VMEM((256, n_keys), jnp.bfloat16),
            pltpu.VMEM((ROPE, n_keys), jnp.bfloat16),
        ],
        compiler_params=pltpu.CompilerParams(vmem_limit_bytes=56 * 1024 * 1024),
        name="attend",
    )(place, query, mine, other, key_up_s, key_up_l, value_up_s, value_up_l)


def merge_kernel(parts, out_s, out_l, out):
    n = parts.shape[0]

    def merged(first, width, stat):
        def stat_of(i, k):
            at = 192 + stat + 3 * k
            return (
                parts[i, :, at : at + 1].astype(jnp.float32)
                + parts[i, :, at + 1 : at + 2].astype(jnp.float32)
            ) + parts[i, :, at + 2 : at + 3].astype(jnp.float32)

        tops = [stat_of(i, 0) for i in range(n)]
        top = tops[0]
        for t in tops[1:]:
            top = jnp.maximum(top, t)
        shares = [stat_of(i, 1) * jnp.exp(tops[i] - top) for i in range(n)]
        total = sum(shares[1:], shares[0])
        acc = 0.0
        for i in range(n):
            acc = acc + parts[i, :, first : first + width].astype(jnp.float32) * (shares[i] / total)
        return acc.astype(jnp.bfloat16)

    large = merged(0, 128, 0)
    small = merged(128, 64, 6)
    mixed = jnp.dot(small, out_s[...], preferred_element_type=jnp.float32) + jnp.dot(
        large, out_l[...], preferred_element_type=jnp.float32
    )
    out[...] = mixed.astype(jnp.bfloat16)


def merge(parts, out_s, out_l):
    vmem = pl.BlockSpec(memory_space=pltpu.VMEM)
    return pl.pallas_call(
        merge_kernel,
        out_shape=jax.ShapeDtypeStruct((parts.shape[1], out_s.shape[1]), jnp.bfloat16),
        in_specs=[vmem] * 3,
        out_specs=vmem,
        name="merge",
    )(parts, out_s, out_l)


def shards(
    residual,
    query_small,
    query_large,
    latent,
    rope_key,
    key_up_small,
    value_up_small,
    key_up_large,
    value_up_large,
    out_small,
    out_large,
    norm_gain,
    gate_weight,
    up_weight,
    down_weight,
):
    n_y = lax.axis_size("y")
    n_x = lax.axis_size("x")
    z = lax.axis_index("z")
    y = lax.axis_index("y")
    x = lax.axis_index("x")
    c = lax.axis_index("c")
    row_count = query_small.shape[0]
    positions = (z * n_y + y) * row_count + jnp.arange(row_count, dtype=jnp.int32)

    query = jnp.concatenate(
        [
            query_large[:, :HEAD_LARGE],
            query_small[:, :HEAD_SMALL],
            rotate(query_small[:, HEAD_SMALL:], positions),
            rotate(query_large[:, HEAD_LARGE:], positions),
        ],
        axis=1,
    )
    width = query.shape[1]
    depth = gate_weight.shape[0]
    groups = row_count // depth
    query_wide = jnp.concatenate(
        [query[depth * g : depth * (g + 1)] for g in range(groups)], axis=1
    )
    cut = gate_weight.shape[1] // n_y
    chunks = jnp.stack(
        [
            jnp.concatenate(
                [query_wide]
                + [w[:, cut * j : cut * (j + 1)] for w in (gate_weight, up_weight, down_weight)],
                axis=1,
            )
            for j in range(n_y)
        ]
    )
    first = exchanged(chunks, "y")
    weights = lax.all_gather(
        first[:, :, width * groups :].reshape(n_y * depth, 3 * cut), "z", axis=0, tiled=True
    )
    queries = jnp.concatenate(
        [
            first[i, :, width * g : width * (g + 1)]
            for i in range(n_y)
            for g in range(groups)
        ],
        axis=0,
    )

    t = x * 2 + c
    turned_key = rotate(rope_key, positions)
    slice_latent = lax.dynamic_slice_in_dim(latent, 32 * t, 32, 1).T
    slice_turned = lax.dynamic_slice_in_dim(turned_key, 8 * x, 8, 1).T
    packed = jnp.concatenate([slice_latent, slice_turned], axis=0)
    along_z = from_everyone(packed, "z")
    mine = from_everyone(along_z, "x")
    other = partner(mine)

    place = jnp.stack([z, y, c]).astype(jnp.int32)
    partial = attention(
        place, queries, mine, other, key_up_small, key_up_large, value_up_small, value_up_large
    )
    parts = exchanged(partial.reshape(n_y, row_count, partial.shape[1]), "y")
    mixed_part = merge(parts, out_small, out_large)
    rows = residual.shape[0]
    d = residual.shape[1]
    tiles = exchanged(mixed_part.reshape(row_count // rows, rows, d), ("x", "c"))
    mixed = jnp.sum(tiles.astype(jnp.float32), axis=0).astype(jnp.bfloat16)
    stream = (residual.astype(jnp.float32) + mixed.astype(jnp.float32)).astype(jnp.bfloat16)
    as_float = stream.astype(jnp.float32)
    normed = as_float * lax.rsqrt(jnp.mean(as_float * as_float, axis=-1, keepdims=True) + norm_eps)
    normed = (normed * norm_gain.astype(jnp.float32)[None, :]).astype(jnp.bfloat16)

    here = from_everyone(normed, ("y", "x")).reshape(n_y * n_x * rows, d)
    there = partner(here)
    gate_full = weights[:, :cut]
    up_full = weights[:, cut : 2 * cut]
    down_full = weights[:, 2 * cut :]

    def mixer(piece):
        gate_part = jnp.dot(piece, gate_full, preferred_element_type=jnp.float32)
        up_part = jnp.dot(piece, up_full, preferred_element_type=jnp.float32)
        hidden = (jax.nn.silu(gate_part) * up_part).astype(jnp.bfloat16)
        return lax.dot_general(hidden, down_full, NT, preferred_element_type=jnp.float32)

    sent = partner(mixer(there).astype(jnp.bfloat16))
    both = (mixer(here) + sent.astype(jnp.float32)).astype(jnp.bfloat16)
    pieces = exchanged(both.reshape(n_y * n_x, rows, d), ("y", "x"))
    channel = jnp.sum(pieces.astype(jnp.float32), axis=0).astype(jnp.bfloat16)
    return (as_float + 0.5 * channel.astype(jnp.float32)).astype(jnp.bfloat16)


def solution(mesh):
    fine = Mesh(mesh.devices.reshape(-1, 4, 4, 2), ("z", "y", "x", "c"))
    sp = ("z", "y")
    tp = ("x", "c")
    both = ("z", "y", "x", "c")
    placed = (
        P(both, None),
        P(sp, tp),
        P(sp, tp),
        P(sp, None),
        P(sp, None),
        P(None, tp),
        P(None, tp),
        P(None, tp),
        P(None, tp),
        P(tp, None),
        P(tp, None),
        P(),
        P(sp, tp),
        P(sp, tp),
        P(sp, tp),
    )
    return jax.shard_map(
        shards, mesh=fine, in_specs=placed, out_specs=P(both, None), check_vma=False
    )
```

```python
import jax
import jax.numpy as jnp
from jax import lax
from jax.experimental import pallas as pl
from jax.experimental.pallas import tpu as pltpu
from jax.sharding import Mesh
from jax.sharding import PartitionSpec as P


HEAD_SMALL = 64
HEAD_LARGE = 128
ROPE = 32
SCALE_SMALL = (HEAD_SMALL + ROPE) ** (-0.5)
SCALE_LARGE = (HEAD_LARGE + ROPE) ** (-0.5)

big_negative = -1e30
rope_base = 500000.0
norm_eps = 1e-06

NT = (((1,), (1,)), ((), ()))
MIB = 1024 * 1024
VMEM = pl.BlockSpec(memory_space=pltpu.VMEM)
SMEM = pl.BlockSpec(memory_space=pltpu.SMEM)


def from_everyone(shard, axis):
    copies = jnp.broadcast_to(shard, (lax.axis_size(axis), *shard.shape))
    return lax.all_to_all(copies, axis, split_axis=0, concat_axis=0, tiled=True)


def exchanged(chunks, axis):
    return lax.all_to_all(chunks, axis, split_axis=0, concat_axis=0, tiled=True)


def partner(x):
    return lax.ppermute(x, "c", [(0, 1), (1, 0)])


def three_parts(v):
    high = v.astype(jnp.bfloat16).astype(jnp.float32)
    rest = v - high
    middle = rest.astype(jnp.bfloat16).astype(jnp.float32)
    low = (rest - middle).astype(jnp.bfloat16).astype(jnp.float32)
    return [high, middle, low]


def weights_kernel(gate, up, down, out):
    cut = gate.shape[1] // 2
    room = out.shape[2] // 3
    depth = gate.shape[0]
    blank = jnp.zeros((depth, room - cut), jnp.float32)
    for k, w in enumerate((gate, up, down)):
        whole = w[...].astype(jnp.float32)
        for j in range(2):
            half = jnp.concatenate([whole[:, cut * j : cut * (j + 1)], blank], axis=1)
            half = half.astype(jnp.bfloat16)
            for i in range(out.shape[0] // 2):
                out[2 * i + j, :, room * k : room * (k + 1)] = half


def pack_weights(gate, up, down, n_y):
    room = -(-(gate.shape[1] // 2) // 128) * 128
    return pl.pallas_call(
        weights_kernel,
        out_shape=jax.ShapeDtypeStruct((n_y, gate.shape[0], 3 * room), jnp.bfloat16),
        in_specs=[VMEM] * 3,
        out_specs=VMEM,
        name="pack_weights",
    )(gate, up, down)


def prepare_kernel(place, small, large, latent, rope_key, table, query, packed, tall):
    cosine = table[:, 0:ROPE]
    sine = table[:, ROPE : 2 * ROPE]

    def turn(v):
        v = v.astype(jnp.float32)
        swapped = jnp.concatenate([v[:, ROPE // 2 :], v[:, : ROPE // 2]], axis=1)
        return v * cosine + swapped * sine

    s = small[...].astype(jnp.float32)
    g = large[...].astype(jnp.float32)
    turned_s = turn(s[:, HEAD_SMALL:]) * SCALE_SMALL
    turned_l = turn(g[:, HEAD_LARGE:]) * SCALE_LARGE
    query[:, 0:128] = large[:, 0:HEAD_LARGE]
    query[:, 128:256] = jnp.concatenate([s[:, :HEAD_SMALL], turned_s, turned_l], axis=1).astype(
        jnp.bfloat16
    )
    tall[0:256, :] = latent[...].astype(jnp.float32).T
    tall[256 : 256 + ROPE, :] = turn(rope_key[...]).astype(jnp.bfloat16).astype(jnp.float32).T
    mine = tall[pl.ds(pl.multiple_of(32 * place[3], 32), 32), :]
    ours = tall[pl.ds(pl.multiple_of(256 + 8 * place[2], 8), 8), :]
    packed[...] = jnp.concatenate([mine, ours], axis=0).astype(jnp.bfloat16)


def prepare(place, small, large, latent, rope_key, table):
    rows = small.shape[0]
    return pl.pallas_call(
        prepare_kernel,
        out_shape=(
            jax.ShapeDtypeStruct((rows, 256), jnp.bfloat16),
            jax.ShapeDtypeStruct((40, rows), jnp.bfloat16),
        ),
        in_specs=[SMEM] + [VMEM] * 5,
        out_specs=(VMEM, VMEM),
        scratch_shapes=[pltpu.VMEM((256 + ROPE, rows), jnp.float32)],
        name="prepare",
    )(place, small, large, latent, rope_key, table)


def absorb_kernel(place, *refs):
    *queries, key_up_s, key_up_l, out = refs
    n_y = len(queries)
    y = place[1]
    row = lax.broadcasted_iota(jnp.int32, (128, 128), 0)
    lane = lax.broadcasted_iota(jnp.int32, (128, 128), 1)
    diagonal = jnp.where(row == lane, 1.0, 0.0)
    pick_lane = lax.broadcasted_iota(jnp.int32, (128, 96), 1)
    for k, query in enumerate(queries):
        j = lax.rem(y - k + n_y, n_y)
        q = query[...]
        own = diagonal if k == 0 else jnp.zeros((128, 128), jnp.float32)
        pick = jnp.where(pick_lane == j, 1.0, 0.0)
        heads = (
            (q[:, 0:128], q[:, 224:256], key_up_l, SCALE_LARGE),
            (q[:, 128:192], q[:, 192:224], key_up_s, SCALE_SMALL),
        )
        for h, (nope, rope, key_up, scale) in enumerate(heads):
            wide = lax.dot_general(nope, key_up[...], NT, preferred_element_type=jnp.float32)
            tail = jnp.concatenate([rope.astype(jnp.float32), pick], axis=1)
            whole = jnp.concatenate([wide * scale, tail, own], axis=1)
            out[j, h, :, :] = whole.astype(jnp.bfloat16)


def absorb(place, queries, key_up_s, key_up_l):
    n_y, rows = len(queries), queries[0].shape[0]
    return pl.pallas_call(
        absorb_kernel,
        out_shape=jax.ShapeDtypeStruct((n_y, 2, rows, 512), jnp.bfloat16),
        in_specs=[SMEM] + [VMEM] * (n_y + 2),
        out_specs=VMEM,
        name="absorb",
    )(place, *queries, key_up_s, key_up_l)


def attention_kernel(place, query, mine, other, value_up_s, value_up_l, out, keys):
    z = place[0]
    y = place[1]
    c = place[4]
    n_x, n_z = mine.shape[0], mine.shape[1]
    n_y = query.shape[0]
    row = lax.broadcasted_iota(jnp.int32, (128, 128), 0)
    lane = lax.broadcasted_iota(jnp.int32, (128, 128), 1)
    for k in range(n_z):
        lanes = pl.ds(128 * k, 128)
        for x in range(n_x):
            here = pl.multiple_of(64 * x + 32 * c, 32)
            there = pl.multiple_of(64 * x + 32 * (1 - c), 32)
            keys[pl.ds(here, 32), lanes] = mine[x, k, 0:32, :]
            keys[pl.ds(there, 32), lanes] = other[x, k, 0:32, :]
        ropes = [mine[x, k, 32:40, :].astype(jnp.float32) for x in range(n_x)]
        keys[256 : 256 + ROPE, lanes] = jnp.concatenate(ropes, axis=0).astype(jnp.bfloat16)
        hidden_from = (k > z) | ((k == z) & (y > row))
        bias = jnp.where(hidden_from & (row < n_y), big_negative, 0.0)
        keys[288:384, lanes] = bias[0:96, :].astype(jnp.bfloat16)
        later = jnp.where((lane > row) & (k == z), big_negative, 0.0)
        keys[384:512, lanes] = later.astype(jnp.bfloat16)
    stat_lane = lax.broadcasted_iota(jnp.int32, (128, 64), 1)

    def head(full, value_up):
        score = jnp.dot(full, keys[...], preferred_element_type=jnp.float32)
        top = jnp.max(score, axis=1, keepdims=True)
        weight = jnp.exp(score - top)
        total = jnp.sum(weight, axis=1, keepdims=True)
        summed = lax.dot_general(
            weight.astype(jnp.bfloat16), keys[0:256, :], NT, preferred_element_type=jnp.float32
        )
        summed = (summed / total).astype(jnp.bfloat16)
        value = jnp.dot(summed, value_up[...], preferred_element_type=jnp.float32)
        return value, top, total

    for j in range(n_y):
        value_l, top_l, total_l = head(query[j, 0], value_up_l)
        value_s, top_s, total_s = head(query[j, 1], value_up_s)
        stats = jnp.zeros((128, 64), jnp.float32)
        parts = three_parts(top_l) + three_parts(total_l) + three_parts(top_s) + three_parts(total_s)
        for i, part in enumerate(parts):
            stats = jnp.where(stat_lane == i, part, stats)
        out[j, :, 0:128] = value_l.astype(jnp.bfloat16)
        out[j, :, 128:256] = jnp.concatenate([value_s, stats], axis=1).astype(jnp.bfloat16)


def attention(place, query, mine, other, value_up_s, value_up_l):
    n_y, _, rows, depth = query.shape
    n_keys = 128 * mine.shape[1]
    return pl.pallas_call(
        attention_kernel,
        out_shape=jax.ShapeDtypeStruct((n_y, rows, 256), jnp.bfloat16),
        in_specs=[SMEM] + [VMEM] * 5,
        out_specs=VMEM,
        scratch_shapes=[pltpu.VMEM((depth, n_keys), jnp.bfloat16)],
        compiler_params=pltpu.CompilerParams(vmem_limit_bytes=24 * MIB),
        name="attend",
    )(place, query, mine, other, value_up_s, value_up_l)


def merge_kernel(parts, out_s, out_l, out):
    n = parts.shape[0]

    def merged(first, width, stat):
        def stat_of(i, k):
            at = 192 + stat + 3 * k
            return (
                parts[i, :, at : at + 1].astype(jnp.float32)
                + parts[i, :, at + 1 : at + 2].astype(jnp.float32)
            ) + parts[i, :, at + 2 : at + 3].astype(jnp.float32)

        tops = [stat_of(i, 0) for i in range(n)]
        top = tops[0]
        for t in tops[1:]:
            top = jnp.maximum(top, t)
        shares = [stat_of(i, 1) * jnp.exp(tops[i] - top) for i in range(n)]
        total = sum(shares[1:], shares[0])
        acc = 0.0
        for i in range(n):
            acc = acc + parts[i, :, first : first + width].astype(jnp.float32) * (shares[i] / total)
        return acc.astype(jnp.bfloat16)

    large = merged(0, 128, 0)
    small = merged(128, 64, 6)
    mixed = jnp.dot(small, out_s[...], preferred_element_type=jnp.float32) + jnp.dot(
        large, out_l[...], preferred_element_type=jnp.float32
    )
    out[...] = mixed.astype(jnp.bfloat16)


def merge(parts, out_s, out_l):
    return pl.pallas_call(
        merge_kernel,
        out_shape=jax.ShapeDtypeStruct((parts.shape[1], out_s.shape[1]), jnp.bfloat16),
        in_specs=[VMEM] * 3,
        out_specs=VMEM,
        name="merge",
    )(parts, out_s, out_l)


def mixer_kernel(here, there, gate_up, down, out_here, out_there, gate, up, hidden):
    step = pl.program_id(0)
    half = pl.num_programs(0) // 2
    rows = here.shape[0]
    room = down.shape[1]

    @pl.when(step == 0)
    def _():
        gate[...] = jnp.zeros_like(gate)
        up[...] = jnp.zeros_like(up)

    @pl.when(step < half)
    def _():
        x = jnp.concatenate([here[...], there[...]], axis=0)
        gate[...] += jnp.dot(x, gate_up[:, 0:room], preferred_element_type=jnp.float32)
        up[...] += jnp.dot(x, gate_up[:, room : 2 * room], preferred_element_type=jnp.float32)

    @pl.when(step == half - 1)
    def _():
        g = gate[...]
        hidden[...] = (g / (1.0 + jnp.exp(-g)) * up[...]).astype(jnp.bfloat16)

    @pl.when(step >= half)
    def _():
        part = lax.dot_general(hidden[...], down[...], NT, preferred_element_type=jnp.float32)
        out_here[...] = part[0:rows, :]
        out_there[...] = part[rows : 2 * rows, :].astype(jnp.bfloat16)


def mixer(here, there, weights):
    rows, d = here.shape
    room = weights.shape[1] // 3
    n = 4
    block = d // n
    return pl.pallas_call(
        mixer_kernel,
        grid=(2 * n,),
        out_shape=(
            jax.ShapeDtypeStruct((rows, d), jnp.float32),
            jax.ShapeDtypeStruct((rows, d), jnp.bfloat16),
        ),
        in_specs=[
            pl.BlockSpec((rows, block), lambda i: (0, jnp.minimum(i, n - 1))),
            pl.BlockSpec((rows, block), lambda i: (0, jnp.minimum(i, n - 1))),
            pl.BlockSpec((block, 2 * room), lambda i: (jnp.minimum(i, n - 1), 0)),
            pl.BlockSpec((block, room), lambda i: (jnp.maximum(i - n, 0), 2)),
        ],
        out_specs=(
            pl.BlockSpec((rows, block), lambda i: (0, jnp.maximum(i - n, 0))),
            pl.BlockSpec((rows, block), lambda i: (0, jnp.maximum(i - n, 0))),
        ),
        scratch_shapes=[
            pltpu.VMEM((2 * rows, room), jnp.float32),
            pltpu.VMEM((2 * rows, room), jnp.float32),
            pltpu.VMEM((2 * rows, room), jnp.bfloat16),
        ],
        compiler_params=pltpu.CompilerParams(vmem_limit_bytes=24 * MIB),
        name="mixer",
    )(here, there, weights, weights)


def shards(
    residual,
    query_small,
    query_large,
    latent,
    rope_key,
    key_up_small,
    value_up_small,
    key_up_large,
    value_up_large,
    out_small,
    out_large,
    norm_gain,
    gate_weight,
    up_weight,
    down_weight,
):
    n_y = lax.axis_size(("yh", "yl"))
    z = lax.axis_index("z")
    y = lax.axis_index(("yh", "yl"))
    x = lax.axis_index("x")
    c = lax.axis_index("c")
    row_count = query_small.shape[0]
    rows, d = residual.shape
    place = jnp.stack([z, y, x, x * 2 + c, c]).astype(jnp.int32)

    chunks = pack_weights(gate_weight, up_weight, down_weight, n_y)
    over_y = exchanged(chunks, ("yh", "yl"))
    weights = lax.all_gather(
        over_y.reshape(-1, over_y.shape[2]), "z", axis=0, tiled=True
    )

    positions = (z * n_y + y) * row_count + jnp.arange(row_count, dtype=jnp.int32)
    inverse = 1.0 / rope_base ** (jnp.arange(0, ROPE, 2, dtype=jnp.float32) / ROPE)
    angles = positions.astype(jnp.float32)[:, None] * inverse[None, :]
    cosine = jnp.cos(angles)
    sine = jnp.sin(angles)
    table = jnp.concatenate([cosine, cosine, -sine, sine], axis=1)
    query, packed = prepare(place, query_small, query_large, latent, rope_key, table)
    along_z = from_everyone(packed, "z")
    queries = [query] + [
        lax.ppermute(query, ("yh", "yl"), [(i, (i + k) % n_y) for i in range(n_y)])
        for k in range(1, n_y)
    ]
    full = absorb(place, queries, key_up_small, key_up_large)
    mine = from_everyone(along_z, "x")
    other = partner(mine)

    partial = attention(place, full, mine, other, value_up_small, value_up_large)
    parts = exchanged(partial, ("yh", "yl"))
    mixed_part = merge(parts, out_small, out_large)
    tiles = exchanged(mixed_part.reshape(row_count // rows, rows, d), ("x", "c"))
    mixed = jnp.sum(tiles.astype(jnp.float32), axis=0).astype(jnp.bfloat16)
    stream = (residual.astype(jnp.float32) + mixed.astype(jnp.float32)).astype(jnp.bfloat16)
    as_float = stream.astype(jnp.float32)
    normed = as_float * lax.rsqrt(jnp.mean(as_float * as_float, axis=-1, keepdims=True) + norm_eps)
    normed = (normed * norm_gain.astype(jnp.float32)[None, :]).astype(jnp.bfloat16)

    here = from_everyone(normed, ("yl", "x")).reshape(-1, d)
    there = partner(here)
    part_here, part_there = mixer(here, there, weights)
    sent = partner(part_there)
    both = (part_here + sent.astype(jnp.float32)).astype(jnp.bfloat16)
    pieces = exchanged(both.reshape(-1, rows, d), ("yl", "x"))
    channel = jnp.sum(pieces.astype(jnp.float32), axis=0).astype(jnp.bfloat16)
    return (as_float + 0.5 * channel.astype(jnp.float32)).astype(jnp.bfloat16)


def solution(mesh):
    fine = Mesh(mesh.devices.reshape(-1, 2, 2, 4, 2), ("z", "yh", "yl", "x", "c"))
    sp = ("z", "yh", "yl")
    tp = ("x", "c")
    both = sp + tp
    placed = (
        P(both, None),
        P(sp, tp),
        P(sp, tp),
        P(sp, None),
        P(sp, None),
        P(None, tp),
        P(None, tp),
        P(None, tp),
        P(None, tp),
        P(tp, None),
        P(tp, None),
        P(),
        P(sp, tp),
        P(sp, tp),
        P(sp, tp),
    )
    return jax.shard_map(
        shards, mesh=fine, in_specs=placed, out_specs=P(both, None), check_vma=False
    )
```

```python
import jax
import jax.numpy as jnp
from jax import lax
from jax.experimental import pallas as pl
from jax.experimental.pallas import tpu as pltpu
from jax.sharding import Mesh
from jax.sharding import PartitionSpec as P


HEAD_SMALL = 64
HEAD_LARGE = 128
ROPE = 32
SCALE_SMALL = (HEAD_SMALL + ROPE) ** (-0.5)
SCALE_LARGE = (HEAD_LARGE + ROPE) ** (-0.5)

big_negative = -1e30
rope_base = 500000.0
norm_eps = 1e-06

NT = (((1,), (1,)), ((), ()))
MIB = 1024 * 1024
VMEM = pl.BlockSpec(memory_space=pltpu.VMEM)
SMEM = pl.BlockSpec(memory_space=pltpu.SMEM)


def where_in(place):
    core = lax.rem(place, 2)
    x = lax.rem(lax.div(place, 2), 4)
    y = lax.rem(lax.div(place, 8), 4)
    return lax.div(place, 32), y, x, core


def from_everyone(shard, axis):
    copies = jnp.broadcast_to(shard, (lax.axis_size(axis), *shard.shape))
    return lax.all_to_all(copies, axis, split_axis=0, concat_axis=0, tiled=True)


def exchanged(chunks, axis):
    return lax.all_to_all(chunks, axis, split_axis=0, concat_axis=0, tiled=True)


def partner(x):
    return lax.ppermute(x, "c", [(0, 1), (1, 0)])


def three_parts(v):
    high = v.astype(jnp.bfloat16).astype(jnp.float32)
    rest = v - high
    middle = rest.astype(jnp.bfloat16).astype(jnp.float32)
    low = (rest - middle).astype(jnp.bfloat16).astype(jnp.float32)
    return [high, middle, low]


def weights_kernel(gate, up, down, out):
    cut = gate.shape[1] // 2
    room = out.shape[2] // 3
    depth = gate.shape[0]
    blank = jnp.zeros((depth, room - cut), jnp.float32)
    for k, w in enumerate((gate, up, down)):
        whole = w[...].astype(jnp.float32)
        for j in range(2):
            half = jnp.concatenate([whole[:, cut * j : cut * (j + 1)], blank], axis=1)
            half = half.astype(jnp.bfloat16)
            for i in range(out.shape[0] // 2):
                out[2 * i + j, :, room * k : room * (k + 1)] = half


def pack_weights(gate, up, down, n_y):
    room = -(-(gate.shape[1] // 2) // 128) * 128
    return pl.pallas_call(
        weights_kernel,
        out_shape=jax.ShapeDtypeStruct((n_y, gate.shape[0], 3 * room), jnp.bfloat16),
        in_specs=[VMEM] * 3,
        out_specs=VMEM,
        name="pack_weights",
    )(gate, up, down)


def prepare_kernel(place, small, large, latent, rope_key, cosine_of, sine_of, query, packed, tall):
    _, _, x, core = where_in(place[0])
    half = ROPE // 2
    cosine = cosine_of[...]
    sine = sine_of[...]

    def turn(v):
        v = v.astype(jnp.float32)
        leading = v[0:half, :]
        trailing = v[half:, :]
        return jnp.concatenate(
            [leading * cosine - trailing * sine, trailing * cosine + leading * sine], axis=0
        )

    tall[0:256, :] = latent[...].astype(jnp.float32).T
    tall[256 : 256 + ROPE, :] = turn(rope_key[...])
    mine = tall[pl.ds(pl.multiple_of(64 * x + 32 * core, 32), 32), :]
    ours = tall[pl.ds(pl.multiple_of(256 + 8 * x, 8), 8), :]
    piece = jnp.concatenate([mine, ours], axis=0).astype(jnp.bfloat16)
    for k in range(packed.shape[0]):
        packed[k] = piece
    upright = jnp.concatenate(
        [
            large[0:HEAD_LARGE, :].astype(jnp.float32),
            small[0:HEAD_SMALL, :].astype(jnp.float32),
            turn(small[HEAD_SMALL:, :]) * SCALE_SMALL,
            turn(large[HEAD_LARGE:, :]) * SCALE_LARGE,
        ],
        axis=0,
    )
    query[...] = upright.T.astype(jnp.bfloat16)


def prepare(place, small, large, latent, rope_key, cosine, sine, n_z):
    rows = latent.shape[0]
    return pl.pallas_call(
        prepare_kernel,
        out_shape=(
            jax.ShapeDtypeStruct((rows, 256), jnp.bfloat16),
            jax.ShapeDtypeStruct((n_z, 40, rows), jnp.bfloat16),
        ),
        in_specs=[SMEM] + [VMEM] * 6,
        out_specs=(VMEM, VMEM),
        scratch_shapes=[pltpu.VMEM((256 + ROPE, rows), jnp.float32)],
        name="prepare",
    )(place, small, large, latent, rope_key, cosine, sine)


def absorb_kernel(place, *refs):
    *queries, key_up_s, key_up_l, out = refs
    n_y = len(queries)
    _, y, _, _ = where_in(place[0])
    row = lax.broadcasted_iota(jnp.int32, (128, 128), 0)
    lane = lax.broadcasted_iota(jnp.int32, (128, 128), 1)
    diagonal = jnp.where(row == lane, 1.0, 0.0)
    pick_lane = lax.broadcasted_iota(jnp.int32, (128, 96), 1)
    for k, query in enumerate(queries):
        j = lax.rem(y - k + n_y, n_y)
        q = query[...]
        own = diagonal if k == 0 else jnp.zeros((128, 128), jnp.float32)
        pick = jnp.where(pick_lane == j, 1.0, 0.0)
        heads = (
            (q[:, 0:128], q[:, 224:256], key_up_l[...].T, SCALE_LARGE),
            (q[:, 128:192], q[:, 192:224], key_up_s[...], SCALE_SMALL),
        )
        for h, (nope, rope, key_up, scale) in enumerate(heads):
            wide = jnp.dot(nope, key_up, preferred_element_type=jnp.float32)
            tail = jnp.concatenate([rope.astype(jnp.float32), pick], axis=1)
            whole = jnp.concatenate([wide * scale, tail, own], axis=1)
            out[j, h, :, :] = whole.astype(jnp.bfloat16)


def absorb(place, queries, key_up_s, key_up_l):
    n_y, rows = len(queries), queries[0].shape[0]
    return pl.pallas_call(
        absorb_kernel,
        out_shape=jax.ShapeDtypeStruct((n_y, 2, rows, 512), jnp.bfloat16),
        in_specs=[SMEM] + [VMEM] * (n_y + 2),
        out_specs=VMEM,
        name="absorb",
    )(place, *queries, key_up_s, key_up_l)


def attention_kernel(place, query, mine, other, value_up_s, value_up_l, out, keys):
    z, y, _, c = where_in(place[0])
    n_x, n_z = mine.shape[0], mine.shape[1]
    n_y = query.shape[0]
    row = lax.broadcasted_iota(jnp.int32, (128, 128), 0)
    lane = lax.broadcasted_iota(jnp.int32, (128, 128), 1)
    for k in range(n_z):
        lanes = pl.ds(128 * k, 128)
        for x in range(n_x):
            here = pl.multiple_of(64 * x + 32 * c, 32)
            there = pl.multiple_of(64 * x + 32 * (1 - c), 32)
            keys[pl.ds(here, 32), lanes] = mine[x, k, 0:32, :]
            keys[pl.ds(there, 32), lanes] = other[x, k, 0:32, :]
        ropes = [mine[x, k, 32:40, :].astype(jnp.float32) for x in range(n_x)]
        keys[256 : 256 + ROPE, lanes] = jnp.concatenate(ropes, axis=0).astype(jnp.bfloat16)
        hidden_from = (k > z) | ((k == z) & (y > row))
        bias = jnp.where(hidden_from & (row < n_y), big_negative, 0.0)
        keys[288:384, lanes] = bias[0:96, :].astype(jnp.bfloat16)
        later = jnp.where((lane > row) & (k == z), big_negative, 0.0)
        keys[384:512, lanes] = later.astype(jnp.bfloat16)
    stat_lane = lax.broadcasted_iota(jnp.int32, (128, 64), 1)

    full = query[...].reshape(n_y * 256, query.shape[3])
    score = jnp.dot(full, keys[...], preferred_element_type=jnp.float32)
    tops = jnp.max(score, axis=1, keepdims=True)
    weight = jnp.exp(score - tops)
    totals = jnp.sum(weight, axis=1, keepdims=True)
    summed = lax.dot_general(
        weight.astype(jnp.bfloat16), keys[0:256, :], NT, preferred_element_type=jnp.float32
    )
    summed = (summed / totals).astype(jnp.bfloat16)
    for j in range(n_y):
        large = slice(256 * j, 256 * j + 128)
        small = slice(256 * j + 128, 256 * j + 256)
        value_l = jnp.dot(summed[large], value_up_l[...], preferred_element_type=jnp.float32)
        value_s = lax.dot_general(
            summed[small], value_up_s[...], NT, preferred_element_type=jnp.float32
        )
        stats = jnp.zeros((128, 64), jnp.float32)
        parts = [
            p for v in (tops[large], totals[large], tops[small], totals[small]) for p in three_parts(v)
        ]
        for i, part in enumerate(parts):
            stats = jnp.where(stat_lane == i, part, stats)
        out[j, :, 0:128] = value_l.astype(jnp.bfloat16)
        out[j, :, 128:256] = jnp.concatenate([value_s, stats], axis=1).astype(jnp.bfloat16)


def attention(place, query, mine, other, value_up_s, value_up_l):
    n_y, _, rows, depth = query.shape
    n_keys = 128 * mine.shape[1]
    return pl.pallas_call(
        attention_kernel,
        out_shape=jax.ShapeDtypeStruct((n_y, rows, 256), jnp.bfloat16),
        in_specs=[SMEM] + [VMEM] * 5,
        out_specs=VMEM,
        scratch_shapes=[pltpu.VMEM((depth, n_keys), jnp.bfloat16)],
        compiler_params=pltpu.CompilerParams(vmem_limit_bytes=36 * MIB),
        name="attend",
    )(place, query, mine, other, value_up_s, value_up_l)


def merge_kernel(parts, out_s, out_l, out):
    n = parts.shape[0]

    def merged(first, width, stat):
        def stat_of(i, k):
            at = 192 + stat + 3 * k
            return (
                parts[i, :, at : at + 1].astype(jnp.float32)
                + parts[i, :, at + 1 : at + 2].astype(jnp.float32)
            ) + parts[i, :, at + 2 : at + 3].astype(jnp.float32)

        tops = [stat_of(i, 0) for i in range(n)]
        top = tops[0]
        for t in tops[1:]:
            top = jnp.maximum(top, t)
        shares = [stat_of(i, 1) * jnp.exp(tops[i] - top) for i in range(n)]
        total = sum(shares[1:], shares[0])
        acc = 0.0
        for i in range(n):
            acc = acc + parts[i, :, first : first + width].astype(jnp.float32) * (shares[i] / total)
        return acc.astype(jnp.bfloat16)

    large = merged(0, 128, 0)
    small = merged(128, 64, 6)
    mixed = jnp.dot(small, out_s[...], preferred_element_type=jnp.float32) + jnp.dot(
        large, out_l[...], preferred_element_type=jnp.float32
    )
    out[...] = mixed.astype(jnp.bfloat16)


def merge(parts, out_s, out_l):
    return pl.pallas_call(
        merge_kernel,
        out_shape=jax.ShapeDtypeStruct((parts.shape[1], out_s.shape[1]), jnp.bfloat16),
        in_specs=[VMEM] * 3,
        out_specs=VMEM,
        name="merge",
    )(parts, out_s, out_l)


def mixer_kernel(here, there, weights, out_here, out_there):
    rows = here.shape[0]
    room = weights.shape[1] // 3
    x = jnp.concatenate([here[...], there[...]], axis=0)
    both = jnp.dot(x, weights[:, 0 : 2 * room], preferred_element_type=jnp.float32)
    gate = both[:, :room]
    hidden = (gate / (1.0 + jnp.exp(-gate)) * both[:, room:]).astype(jnp.bfloat16)
    part = lax.dot_general(hidden, weights[:, 2 * room :], NT, preferred_element_type=jnp.float32)
    out_here[...] = part[0:rows, :]
    out_there[...] = part[rows : 2 * rows, :].astype(jnp.bfloat16)


def mixer(here, there, weights):
    return pl.pallas_call(
        mixer_kernel,
        out_shape=(
            jax.ShapeDtypeStruct(here.shape, jnp.float32),
            jax.ShapeDtypeStruct(here.shape, jnp.bfloat16),
        ),
        in_specs=[VMEM] * 3,
        out_specs=(VMEM, VMEM),
        compiler_params=pltpu.CompilerParams(vmem_limit_bytes=24 * MIB),
        name="mixer",
    )(here, there, weights)


def shards(
    residual,
    query_small,
    query_large,
    latent,
    rope_key,
    key_up_small,
    value_up_small,
    key_up_large,
    value_up_large,
    out_small,
    out_large,
    norm_gain,
    gate_weight,
    up_weight,
    down_weight,
):
    n_y = lax.axis_size(("yh", "yl"))
    z = lax.axis_index("z")
    y = lax.axis_index(("yh", "yl"))
    x = lax.axis_index("x")
    c = lax.axis_index("c")
    row_count = query_small.shape[0]
    rows, d = residual.shape
    place = (((z * n_y + y) * lax.axis_size("x") + x) * 2 + c).astype(jnp.int32).reshape(1)

    chunks = pack_weights(gate_weight, up_weight, down_weight, n_y)
    over_y = exchanged(chunks, ("yh", "yl"))
    weights = lax.all_gather(
        over_y.reshape(-1, over_y.shape[2]), "z", axis=0, tiled=True
    )

    positions = (z * n_y + y) * row_count + jnp.arange(row_count, dtype=jnp.int32)
    inverse = 1.0 / rope_base ** (jnp.arange(0, ROPE, 2, dtype=jnp.float32) / ROPE)
    angles = positions.astype(jnp.float32)[None, :] * inverse[:, None]
    query, packed = prepare(
        place,
        query_small.T,
        query_large.T,
        latent,
        rope_key.T,
        jnp.cos(angles),
        jnp.sin(angles),
        lax.axis_size("z"),
    )
    along_z = exchanged(packed, "z")
    queries = [query] + [
        lax.ppermute(query, ("yh", "yl"), [(i, (i + k) % n_y) for i in range(n_y)])
        for k in range(1, n_y)
    ]
    full = absorb(place, queries, key_up_small.T, key_up_large)
    mine = from_everyone(along_z, "x")
    other = partner(mine)

    partial = attention(place, full, mine, other, value_up_small.T, value_up_large)
    parts = exchanged(partial, ("yh", "yl"))
    mixed_part = merge(parts, out_small, out_large)
    tiles = exchanged(mixed_part.reshape(row_count // rows, rows, d), ("x", "c"))
    mixed = jnp.sum(tiles.astype(jnp.float32), axis=0).astype(jnp.bfloat16)
    stream = (residual.astype(jnp.float32) + mixed.astype(jnp.float32)).astype(jnp.bfloat16)
    as_float = stream.astype(jnp.float32)
    normed = as_float * lax.rsqrt(jnp.mean(as_float * as_float, axis=-1, keepdims=True) + norm_eps)
    normed = (normed * norm_gain.astype(jnp.float32)[None, :]).astype(jnp.bfloat16)

    here = from_everyone(normed, ("yl", "x")).reshape(-1, d)
    here, weights = lax.optimization_barrier((here, weights))
    there = partner(here)
    part_here, part_there = mixer(here, there, weights)
    sent = partner(part_there)
    both = (part_here + sent.astype(jnp.float32)).astype(jnp.bfloat16)
    pieces = exchanged(both.reshape(-1, rows, d), ("yl", "x"))
    channel = jnp.sum(pieces.astype(jnp.float32), axis=0).astype(jnp.bfloat16)
    return (as_float + 0.5 * channel.astype(jnp.float32)).astype(jnp.bfloat16)


def solution(mesh):
    fine = Mesh(mesh.devices.reshape(-1, 2, 2, 4, 2), ("z", "yh", "yl", "x", "c"))
    sp = ("z", "yh", "yl")
    tp = ("x", "c")
    both = sp + tp
    placed = (
        P(both, None),
        P(sp, tp),
        P(sp, tp),
        P(sp, None),
        P(sp, None),
        P(None, tp),
        P(None, tp),
        P(None, tp),
        P(None, tp),
        P(tp, None),
        P(tp, None),
        P(),
        P(sp, tp),
        P(sp, tp),
        P(sp, tp),
    )
    return jax.shard_map(
        shards, mesh=fine, in_specs=placed, out_specs=P(both, None), check_vma=False
    )
```

```python
import jax
import jax.numpy as jnp
from jax import lax
from jax.experimental import pallas as pl
from jax.experimental.pallas import tpu as pltpu
from jax.sharding import Mesh
from jax.sharding import PartitionSpec as P


HEAD_SMALL = 64
HEAD_LARGE = 128
ROPE = 32
SCALE_SMALL = (HEAD_SMALL + ROPE) ** (-0.5)
SCALE_LARGE = (HEAD_LARGE + ROPE) ** (-0.5)

big_negative = -1e30
rope_base = 500000.0
norm_eps = 1e-06

NT = (((1,), (1,)), ((), ()))
MIB = 1024 * 1024
VMEM = pl.BlockSpec(memory_space=pltpu.VMEM)
SMEM = pl.BlockSpec(memory_space=pltpu.SMEM)


def where_in(place):
    core = lax.rem(place, 2)
    x = lax.rem(lax.div(place, 2), 4)
    y = lax.rem(lax.div(place, 8), 4)
    return lax.div(place, 32), y, x, core


def from_everyone(shard, axis):
    copies = jnp.broadcast_to(shard, (lax.axis_size(axis), *shard.shape))
    return lax.all_to_all(copies, axis, split_axis=0, concat_axis=0, tiled=True)


def exchanged(chunks, axis):
    return lax.all_to_all(chunks, axis, split_axis=0, concat_axis=0, tiled=True)


def partner(x):
    return lax.ppermute(x, "c", [(0, 1), (1, 0)])


def three_parts(v):
    high = v.astype(jnp.bfloat16).astype(jnp.float32)
    rest = v - high
    middle = rest.astype(jnp.bfloat16).astype(jnp.float32)
    low = (rest - middle).astype(jnp.bfloat16).astype(jnp.float32)
    return [high, middle, low]


def weights_kernel(gate, up, down, out):
    cut = gate.shape[1] // 2
    room = out.shape[2] // 3
    depth = gate.shape[0]
    blank = jnp.zeros((depth, room - cut), jnp.float32)
    for k, w in enumerate((gate, up, down)):
        whole = w[...].astype(jnp.float32)
        for j in range(2):
            half = jnp.concatenate([whole[:, cut * j : cut * (j + 1)], blank], axis=1)
            half = half.astype(jnp.bfloat16)
            for i in range(out.shape[0] // 2):
                out[2 * i + j, :, room * k : room * (k + 1)] = half


def pack_weights(gate, up, down, n_y):
    room = -(-(gate.shape[1] // 2) // 128) * 128
    return pl.pallas_call(
        weights_kernel,
        out_shape=jax.ShapeDtypeStruct((n_y, gate.shape[0], 3 * room), jnp.bfloat16),
        in_specs=[VMEM] * 3,
        out_specs=VMEM,
        compiler_params=pltpu.CompilerParams(vmem_limit_bytes=4 * MIB),
        name="pack_weights",
    )(gate, up, down)


def prepare_kernel(place, small, large, latent, rope_key, cosine_of, sine_of, query, packed, tall):
    _, _, x, core = where_in(place[0])
    half = ROPE // 2
    cosine = cosine_of[...]
    sine = sine_of[...]

    def turn(v):
        v = v.astype(jnp.float32)
        leading = v[0:half, :]
        trailing = v[half:, :]
        return jnp.concatenate(
            [leading * cosine - trailing * sine, trailing * cosine + leading * sine], axis=0
        )

    tall[0:256, :] = latent[...].astype(jnp.float32).T
    tall[256 : 256 + ROPE, :] = turn(rope_key[...])
    mine = tall[pl.ds(pl.multiple_of(64 * x + 32 * core, 32), 32), :]
    ours = tall[pl.ds(pl.multiple_of(256 + 8 * x, 8), 8), :]
    piece = jnp.concatenate([mine, ours], axis=0).astype(jnp.bfloat16)
    for k in range(packed.shape[0]):
        packed[k] = piece
    upright = jnp.concatenate(
        [
            large[0:HEAD_LARGE, :].astype(jnp.float32),
            small[0:HEAD_SMALL, :].astype(jnp.float32),
            turn(small[HEAD_SMALL:, :]) * SCALE_SMALL,
            turn(large[HEAD_LARGE:, :]) * SCALE_LARGE,
        ],
        axis=0,
    )
    query[...] = upright.T.astype(jnp.bfloat16)


def prepare(place, small, large, latent, rope_key, cosine, sine, n_z):
    rows = latent.shape[0]
    return pl.pallas_call(
        prepare_kernel,
        out_shape=(
            jax.ShapeDtypeStruct((rows, 256), jnp.bfloat16),
            jax.ShapeDtypeStruct((n_z, 40, rows), jnp.bfloat16),
        ),
        in_specs=[SMEM] + [VMEM] * 6,
        out_specs=(VMEM, VMEM),
        scratch_shapes=[pltpu.VMEM((256 + ROPE, rows), jnp.float32)],
        compiler_params=pltpu.CompilerParams(vmem_limit_bytes=4 * MIB),
        name="prepare",
    )(place, small, large, latent, rope_key, cosine, sine)


def join_kernel(place, *refs):
    *queries, out = refs
    n_y = len(queries)
    _, y, _, _ = where_in(place[0])
    for k, query in enumerate(queries):
        out[lax.rem(y - k + n_y, n_y)] = query[...]


def join(place, queries):
    return pl.pallas_call(
        join_kernel,
        out_shape=jax.ShapeDtypeStruct((len(queries), *queries[0].shape), jnp.bfloat16),
        in_specs=[SMEM] + [VMEM] * len(queries),
        out_specs=VMEM,
        compiler_params=pltpu.CompilerParams(vmem_limit_bytes=4 * MIB),
        name="join",
    )(place, *queries)


def absorb_kernel(place, query, key_up_s, key_up_l, out):
    n_y = query.shape[0]
    _, y, _, _ = where_in(place[0])
    row = lax.broadcasted_iota(jnp.int32, (128, 128), 0)
    lane = lax.broadcasted_iota(jnp.int32, (128, 128), 1)
    diagonal = jnp.where(row == lane, 1.0, 0.0)
    pick_lane = lax.broadcasted_iota(jnp.int32, (128, 96), 1)
    key_up_large = key_up_l[...].T
    for j in range(n_y):
        q = query[j]
        own = jnp.where(y == j, diagonal, 0.0)
        pick = jnp.where(pick_lane == j, 1.0, 0.0)
        heads = (
            (q[:, 0:128], q[:, 224:256], key_up_large, SCALE_LARGE),
            (q[:, 128:192], q[:, 192:224], key_up_s[...], SCALE_SMALL),
        )
        for h, (nope, rope, key_up, scale) in enumerate(heads):
            wide = jnp.dot(nope, key_up, preferred_element_type=jnp.float32)
            tail = jnp.concatenate([rope.astype(jnp.float32), pick], axis=1)
            whole = jnp.concatenate([wide * scale, tail, own], axis=1)
            out[j, h, :, :] = whole.astype(jnp.bfloat16)


def absorb(place, query, key_up_s, key_up_l):
    n_y, rows = query.shape[:2]
    return pl.pallas_call(
        absorb_kernel,
        out_shape=jax.ShapeDtypeStruct((n_y, 2, rows, 512), jnp.bfloat16),
        in_specs=[SMEM] + [VMEM] * 3,
        out_specs=VMEM,
        compiler_params=pltpu.CompilerParams(vmem_limit_bytes=8 * MIB),
        name="absorb",
    )(place, query, key_up_s, key_up_l)


def attention_kernel(place, query, mine, other, value_up_s, value_up_l, out, keys):
    z, y, _, c = where_in(place[0])
    n_x, n_z = mine.shape[0], mine.shape[1]
    n_y = query.shape[0]
    row = lax.broadcasted_iota(jnp.int32, (128, 128), 0)
    lane = lax.broadcasted_iota(jnp.int32, (128, 128), 1)
    for k in range(n_z):
        lanes = pl.ds(128 * k, 128)
        for x in range(n_x):
            here = pl.multiple_of(64 * x + 32 * c, 32)
            there = pl.multiple_of(64 * x + 32 * (1 - c), 32)
            keys[pl.ds(here, 32), lanes] = mine[x, k, 0:32, :]
            keys[pl.ds(there, 32), lanes] = other[x, k, 0:32, :]
        ropes = [mine[x, k, 32:40, :].astype(jnp.float32) for x in range(n_x)]
        keys[256 : 256 + ROPE, lanes] = jnp.concatenate(ropes, axis=0).astype(jnp.bfloat16)
        hidden_from = (k > z) | ((k == z) & (y > row))
        bias = jnp.where(hidden_from & (row < n_y), big_negative, 0.0)
        keys[288:384, lanes] = bias[0:96, :].astype(jnp.bfloat16)
        later = jnp.where((lane > row) & (k == z), big_negative, 0.0)
        keys[384:512, lanes] = later.astype(jnp.bfloat16)
    stat_lane = lax.broadcasted_iota(jnp.int32, (128, 64), 1)

    full = query[...].reshape(n_y * 256, query.shape[3])
    score = jnp.dot(full, keys[...], preferred_element_type=jnp.float32)
    tops = jnp.max(score, axis=1, keepdims=True)
    weight = jnp.exp(score - tops)
    totals = jnp.sum(weight, axis=1, keepdims=True)
    summed = lax.dot_general(
        weight.astype(jnp.bfloat16), keys[0:256, :], NT, preferred_element_type=jnp.float32
    )
    summed = (summed / totals).astype(jnp.bfloat16)
    for j in range(n_y):
        large = slice(256 * j, 256 * j + 128)
        small = slice(256 * j + 128, 256 * j + 256)
        value_l = jnp.dot(summed[large], value_up_l[...], preferred_element_type=jnp.float32)
        value_s = lax.dot_general(
            summed[small], value_up_s[...], NT, preferred_element_type=jnp.float32
        )
        stats = jnp.zeros((128, 64), jnp.float32)
        parts = [
            p for v in (tops[large], totals[large], tops[small], totals[small]) for p in three_parts(v)
        ]
        for i, part in enumerate(parts):
            stats = jnp.where(stat_lane == i, part, stats)
        out[j, :, 0:128] = value_l.astype(jnp.bfloat16)
        out[j, :, 128:256] = jnp.concatenate([value_s, stats], axis=1).astype(jnp.bfloat16)


def attention(place, query, mine, other, value_up_s, value_up_l):
    n_y, _, rows, depth = query.shape
    n_keys = 128 * mine.shape[1]
    return pl.pallas_call(
        attention_kernel,
        out_shape=jax.ShapeDtypeStruct((n_y, rows, 256), jnp.bfloat16),
        in_specs=[SMEM] + [VMEM] * 5,
        out_specs=VMEM,
        scratch_shapes=[pltpu.VMEM((depth, n_keys), jnp.bfloat16)],
        compiler_params=pltpu.CompilerParams(vmem_limit_bytes=36 * MIB),
        name="attend",
    )(place, query, mine, other, value_up_s, value_up_l)


def merge_kernel(parts, out_s, out_l, out):
    n = parts.shape[0]

    def merged(first, width, stat):
        def stat_of(i, k):
            at = 192 + stat + 3 * k
            return (
                parts[i, :, at : at + 1].astype(jnp.float32)
                + parts[i, :, at + 1 : at + 2].astype(jnp.float32)
            ) + parts[i, :, at + 2 : at + 3].astype(jnp.float32)

        tops = [stat_of(i, 0) for i in range(n)]
        top = tops[0]
        for t in tops[1:]:
            top = jnp.maximum(top, t)
        shares = [stat_of(i, 1) * jnp.exp(tops[i] - top) for i in range(n)]
        total = sum(shares[1:], shares[0])
        acc = 0.0
        for i in range(n):
            acc = acc + parts[i, :, first : first + width].astype(jnp.float32) * (shares[i] / total)
        return acc.astype(jnp.bfloat16)

    large = merged(0, 128, 0)
    small = merged(128, 64, 6)
    mixed = jnp.dot(small, out_s[...], preferred_element_type=jnp.float32) + jnp.dot(
        large, out_l[...], preferred_element_type=jnp.float32
    )
    out[...] = mixed.astype(jnp.bfloat16)


def merge(parts, out_s, out_l):
    return pl.pallas_call(
        merge_kernel,
        out_shape=jax.ShapeDtypeStruct((parts.shape[1], out_s.shape[1]), jnp.bfloat16),
        in_specs=[VMEM] * 3,
        out_specs=VMEM,
        compiler_params=pltpu.CompilerParams(vmem_limit_bytes=8 * MIB),
        name="merge",
    )(parts, out_s, out_l)


def mixer_kernel(here, there, weights, out_here, out_there, gate_up, down, arrived):
    rows = here.shape[0]
    d = weights.shape[0]
    room = weights.shape[1] // 3
    pieces = arrived.shape[0] - 1
    block = d // pieces
    copies = [
        pltpu.make_async_copy(
            weights.at[pl.ds(block * i, block), pl.ds(0, 2 * room)],
            gate_up.at[pl.ds(block * i, block), :],
            arrived.at[i],
        )
        for i in range(pieces)
    ]
    copies.append(
        pltpu.make_async_copy(weights.at[:, pl.ds(2 * room, room)], down, arrived.at[pieces])
    )
    for copy in copies:
        copy.start()
    x = jnp.concatenate([here[...], there[...]], axis=0)
    both = None
    for i in range(pieces):
        copies[i].wait()
        term = jnp.dot(
            x[:, block * i : block * (i + 1)],
            gate_up[block * i : block * (i + 1), :],
            preferred_element_type=jnp.float32,
        )
        both = term if both is None else both + term
    gate = both[:, :room]
    hidden = (gate / (1.0 + jnp.exp(-gate)) * both[:, room:]).astype(jnp.bfloat16)
    copies[pieces].wait()
    part = lax.dot_general(hidden, down[...], NT, preferred_element_type=jnp.float32)
    out_here[...] = part[0:rows, :]
    out_there[...] = part[rows : 2 * rows, :].astype(jnp.bfloat16)


def mixer(here, there, weights):
    d = weights.shape[0]
    room = weights.shape[1] // 3
    return pl.pallas_call(
        mixer_kernel,
        out_shape=(
            jax.ShapeDtypeStruct(here.shape, jnp.float32),
            jax.ShapeDtypeStruct(here.shape, jnp.bfloat16),
        ),
        in_specs=[VMEM] * 2 + [pl.BlockSpec(memory_space=pltpu.HBM)],
        out_specs=(VMEM, VMEM),
        scratch_shapes=[
            pltpu.VMEM((d, 2 * room), jnp.bfloat16),
            pltpu.VMEM((d, room), jnp.bfloat16),
            pltpu.SemaphoreType.DMA((5,)),
        ],
        compiler_params=pltpu.CompilerParams(vmem_limit_bytes=52 * MIB),
        name="mixer",
    )(here, there, weights)


def shards(
    residual,
    query_small,
    query_large,
    latent,
    rope_key,
    key_up_small,
    value_up_small,
    key_up_large,
    value_up_large,
    out_small,
    out_large,
    norm_gain,
    gate_weight,
    up_weight,
    down_weight,
):
    n_y = lax.axis_size(("yh", "yl"))
    z = lax.axis_index("z")
    y = lax.axis_index(("yh", "yl"))
    x = lax.axis_index("x")
    c = lax.axis_index("c")
    row_count = query_small.shape[0]
    rows, d = residual.shape
    place = (((z * n_y + y) * lax.axis_size("x") + x) * 2 + c).astype(jnp.int32).reshape(1)

    chunks = pack_weights(gate_weight, up_weight, down_weight, n_y)
    over_y = exchanged(chunks, ("yh", "yl"))
    weights = lax.all_gather(
        over_y.reshape(-1, over_y.shape[2]), "z", axis=0, tiled=True
    )

    positions = (z * n_y + y) * row_count + jnp.arange(row_count, dtype=jnp.int32)
    inverse = 1.0 / rope_base ** (jnp.arange(0, ROPE, 2, dtype=jnp.float32) / ROPE)
    angles = positions.astype(jnp.float32)[None, :] * inverse[:, None]
    query, packed = prepare(
        place,
        query_small.T,
        query_large.T,
        latent,
        rope_key.T,
        jnp.cos(angles),
        jnp.sin(angles),
        lax.axis_size("z"),
    )
    along_z = exchanged(packed, "z")
    queries = [query] + [
        lax.ppermute(query, ("yh", "yl"), [(i, (i + k) % n_y) for i in range(n_y)])
        for k in range(1, n_y)
    ]
    full = absorb(place, join(place, queries), key_up_small.T, key_up_large)
    mine = from_everyone(along_z, "x")
    other = partner(mine)

    partial = attention(place, full, mine, other, value_up_small.T, value_up_large)
    parts = exchanged(partial, ("yh", "yl"))
    mixed_part = merge(parts, out_small, out_large)
    tiles = exchanged(mixed_part.reshape(row_count // rows, rows, d), ("x", "c"))
    mixed = jnp.sum(tiles.astype(jnp.float32), axis=0).astype(jnp.bfloat16)
    stream = (residual.astype(jnp.float32) + mixed.astype(jnp.float32)).astype(jnp.bfloat16)
    as_float = stream.astype(jnp.float32)
    normed = as_float * lax.rsqrt(jnp.mean(as_float * as_float, axis=-1, keepdims=True) + norm_eps)
    normed = (normed * norm_gain.astype(jnp.float32)[None, :]).astype(jnp.bfloat16)

    here = from_everyone(normed, ("yl", "x")).reshape(-1, d)
    here, weights = lax.optimization_barrier((here, weights))
    there = partner(here)
    part_here, part_there = mixer(here, there, weights)
    sent = partner(part_there)
    both = (part_here + sent.astype(jnp.float32)).astype(jnp.bfloat16)
    pieces = exchanged(both.reshape(-1, rows, d), ("yl", "x"))
    channel = jnp.sum(pieces.astype(jnp.float32), axis=0).astype(jnp.bfloat16)
    return (as_float + 0.5 * channel.astype(jnp.float32)).astype(jnp.bfloat16)


def solution(mesh):
    fine = Mesh(mesh.devices.reshape(-1, 2, 2, 4, 2), ("z", "yh", "yl", "x", "c"))
    sp = ("z", "yh", "yl")
    tp = ("x", "c")
    both = sp + tp
    placed = (
        P(both, None),
        P(sp, tp),
        P(sp, tp),
        P(sp, None),
        P(sp, None),
        P(None, tp),
        P(None, tp),
        P(None, tp),
        P(None, tp),
        P(tp, None),
        P(tp, None),
        P(),
        P(sp, tp),
        P(sp, tp),
        P(sp, tp),
    )
    return jax.shard_map(
        shards, mesh=fine, in_specs=placed, out_specs=P(both, None), check_vma=False
    )
```

```python
import jax
import jax.numpy as jnp
from jax import lax
from jax.experimental import pallas as pl
from jax.experimental.pallas import tpu as pltpu
from jax.sharding import Mesh
from jax.sharding import PartitionSpec as P


HEAD_SMALL = 64
HEAD_LARGE = 128
ROPE = 32
SCALE_SMALL = (HEAD_SMALL + ROPE) ** (-0.5)
SCALE_LARGE = (HEAD_LARGE + ROPE) ** (-0.5)

big_negative = -1e30
rope_base = 500000.0
norm_eps = 1e-06

NT = (((1,), (1,)), ((), ()))
MIB = 1024 * 1024
VMEM = pl.BlockSpec(memory_space=pltpu.VMEM)
SMEM = pl.BlockSpec(memory_space=pltpu.SMEM)


def where_in(place):
    core = lax.rem(place, 2)
    x = lax.rem(lax.div(place, 2), 4)
    y = lax.rem(lax.div(place, 8), 4)
    return lax.div(place, 32), y, x, core


def from_everyone(shard, axis):
    copies = jnp.broadcast_to(shard, (lax.axis_size(axis), *shard.shape))
    return lax.all_to_all(copies, axis, split_axis=0, concat_axis=0, tiled=True)


def exchanged(chunks, axis):
    return lax.all_to_all(chunks, axis, split_axis=0, concat_axis=0, tiled=True)


def partner(x):
    return lax.ppermute(x, "c", [(0, 1), (1, 0)])


def three_parts(v):
    high = v.astype(jnp.bfloat16).astype(jnp.float32)
    rest = v - high
    middle = rest.astype(jnp.bfloat16).astype(jnp.float32)
    low = (rest - middle).astype(jnp.bfloat16).astype(jnp.float32)
    return [high, middle, low]


def weights_kernel(gate, up, down, out):
    cut = gate.shape[1] // 2
    room = out.shape[2] // 3
    depth = gate.shape[0]
    blank = jnp.zeros((depth, room - cut), jnp.float32)
    for k, w in enumerate((gate, up, down)):
        whole = w[...].astype(jnp.float32)
        for j in range(2):
            half = jnp.concatenate([whole[:, cut * j : cut * (j + 1)], blank], axis=1)
            half = half.astype(jnp.bfloat16)
            for i in range(out.shape[0] // 2):
                out[2 * i + j, :, room * k : room * (k + 1)] = half


def pack_weights(gate, up, down, n_y):
    room = -(-(gate.shape[1] // 2) // 128) * 128
    return pl.pallas_call(
        weights_kernel,
        out_shape=jax.ShapeDtypeStruct((n_y, gate.shape[0], 3 * room), jnp.bfloat16),
        in_specs=[VMEM] * 3,
        out_specs=VMEM,
        name="pack_weights",
    )(gate, up, down)


def prepare_kernel(place, small, large, latent, rope_key, cosine_of, sine_of, query, packed, tall):
    _, _, x, core = where_in(place[0])
    half = ROPE // 2
    cosine = cosine_of[...]
    sine = sine_of[...]

    def turn(v):
        v = v.astype(jnp.float32)
        leading = v[0:half, :]
        trailing = v[half:, :]
        return jnp.concatenate(
            [leading * cosine - trailing * sine, trailing * cosine + leading * sine], axis=0
        )

    tall[0:256, :] = latent[...].astype(jnp.float32).T
    tall[256 : 256 + ROPE, :] = turn(rope_key[...])
    mine = tall[pl.ds(pl.multiple_of(64 * x + 32 * core, 32), 32), :]
    ours = tall[pl.ds(pl.multiple_of(256 + 8 * x, 8), 8), :]
    piece = jnp.concatenate([mine, ours], axis=0).astype(jnp.bfloat16)
    for k in range(packed.shape[0]):
        packed[k] = piece
    upright = jnp.concatenate(
        [
            large[0:HEAD_LARGE, :].astype(jnp.float32),
            small[0:HEAD_SMALL, :].astype(jnp.float32),
            turn(small[HEAD_SMALL:, :]) * SCALE_SMALL,
            turn(large[HEAD_LARGE:, :]) * SCALE_LARGE,
        ],
        axis=0,
    )
    query[...] = upright.T.astype(jnp.bfloat16)


def prepare(place, small, large, latent, rope_key, cosine, sine, n_z):
    rows = latent.shape[0]
    return pl.pallas_call(
        prepare_kernel,
        out_shape=(
            jax.ShapeDtypeStruct((rows, 256), jnp.bfloat16),
            jax.ShapeDtypeStruct((n_z, 40, rows), jnp.bfloat16),
        ),
        in_specs=[SMEM] + [VMEM] * 6,
        out_specs=(VMEM, VMEM),
        scratch_shapes=[pltpu.VMEM((256 + ROPE, rows), jnp.float32)],
        compiler_params=pltpu.CompilerParams(vmem_limit_bytes=4 * MIB),
        name="prepare",
    )(place, small, large, latent, rope_key, cosine, sine)


def join_kernel(place, *refs):
    *queries, out = refs
    n_y = len(queries)
    _, y, _, _ = where_in(place[0])
    for k, query in enumerate(queries):
        out[lax.rem(y - k + n_y, n_y)] = query[...]


def join(place, queries):
    return pl.pallas_call(
        join_kernel,
        out_shape=jax.ShapeDtypeStruct((len(queries), *queries[0].shape), jnp.bfloat16),
        in_specs=[SMEM] + [VMEM] * len(queries),
        out_specs=VMEM,
        compiler_params=pltpu.CompilerParams(vmem_limit_bytes=4 * MIB),
        name="join",
    )(place, *queries)


def absorb_kernel(place, query, key_up_s, key_up_l, out):
    n_y = query.shape[0]
    _, y, _, _ = where_in(place[0])
    row = lax.broadcasted_iota(jnp.int32, (128, 128), 0)
    lane = lax.broadcasted_iota(jnp.int32, (128, 128), 1)
    diagonal = jnp.where(row == lane, 1.0, 0.0)
    pick_lane = lax.broadcasted_iota(jnp.int32, (128, 96), 1)
    key_up_large = key_up_l[...].T
    for j in range(n_y):
        q = query[j]
        own = jnp.where(y == j, diagonal, 0.0)
        pick = jnp.where(pick_lane == j, 1.0, 0.0)
        heads = (
            (q[:, 0:128], q[:, 224:256], key_up_large, SCALE_LARGE),
            (q[:, 128:192], q[:, 192:224], key_up_s[...], SCALE_SMALL),
        )
        for h, (nope, rope, key_up, scale) in enumerate(heads):
            wide = jnp.dot(nope, key_up, preferred_element_type=jnp.float32)
            tail = jnp.concatenate([rope.astype(jnp.float32), pick], axis=1)
            whole = jnp.concatenate([wide * scale, tail, own], axis=1)
            out[j, h, :, :] = whole.astype(jnp.bfloat16)


def absorb(place, query, key_up_s, key_up_l):
    n_y, rows = query.shape[:2]
    return pl.pallas_call(
        absorb_kernel,
        out_shape=jax.ShapeDtypeStruct((n_y, 2, rows, 512), jnp.bfloat16),
        in_specs=[SMEM] + [VMEM] * 3,
        out_specs=VMEM,
        compiler_params=pltpu.CompilerParams(vmem_limit_bytes=8 * MIB),
        name="absorb",
    )(place, query, key_up_s, key_up_l)


def attention_kernel(place, query, mine, other, value_up_s, value_up_l, out, keys):
    z, y, _, c = where_in(place[0])
    n_x, n_z = mine.shape[0], mine.shape[1]
    n_y = query.shape[0]
    row = lax.broadcasted_iota(jnp.int32, (128, 128), 0)
    lane = lax.broadcasted_iota(jnp.int32, (128, 128), 1)
    for k in range(n_z):
        lanes = pl.ds(128 * k, 128)
        for x in range(n_x):
            here = pl.multiple_of(64 * x + 32 * c, 32)
            there = pl.multiple_of(64 * x + 32 * (1 - c), 32)
            keys[pl.ds(here, 32), lanes] = mine[x, k, 0:32, :]
            keys[pl.ds(there, 32), lanes] = other[x, k, 0:32, :]
        ropes = [mine[x, k, 32:40, :].astype(jnp.float32) for x in range(n_x)]
        keys[256 : 256 + ROPE, lanes] = jnp.concatenate(ropes, axis=0).astype(jnp.bfloat16)
        hidden_from = (k > z) | ((k == z) & (y > row))
        bias = jnp.where(hidden_from & (row < n_y), big_negative, 0.0)
        keys[288:384, lanes] = bias[0:96, :].astype(jnp.bfloat16)
        later = jnp.where((lane > row) & (k == z), big_negative, 0.0)
        keys[384:512, lanes] = later.astype(jnp.bfloat16)
    stat_lane = lax.broadcasted_iota(jnp.int32, (128, 64), 1)

    full = query[...].reshape(n_y * 256, query.shape[3])
    score = jnp.dot(full, keys[...], preferred_element_type=jnp.float32)
    tops = jnp.max(score, axis=1, keepdims=True)
    weight = jnp.exp(score - tops)
    totals = jnp.sum(weight, axis=1, keepdims=True)
    summed = lax.dot_general(
        weight.astype(jnp.bfloat16), keys[0:256, :], NT, preferred_element_type=jnp.float32
    )
    summed = (summed / totals).astype(jnp.bfloat16)
    for j in range(n_y):
        large = slice(256 * j, 256 * j + 128)
        small = slice(256 * j + 128, 256 * j + 256)
        value_l = jnp.dot(summed[large], value_up_l[...], preferred_element_type=jnp.float32)
        value_s = lax.dot_general(
            summed[small], value_up_s[...], NT, preferred_element_type=jnp.float32
        )
        stats = jnp.zeros((128, 64), jnp.float32)
        parts = [
            p for v in (tops[large], totals[large], tops[small], totals[small]) for p in three_parts(v)
        ]
        for i, part in enumerate(parts):
            stats = jnp.where(stat_lane == i, part, stats)
        out[j, :, 0:128] = value_l.astype(jnp.bfloat16)
        out[j, :, 128:256] = jnp.concatenate([value_s, stats], axis=1).astype(jnp.bfloat16)


def attention(place, query, mine, other, value_up_s, value_up_l):
    n_y, _, rows, depth = query.shape
    n_keys = 128 * mine.shape[1]
    return pl.pallas_call(
        attention_kernel,
        out_shape=jax.ShapeDtypeStruct((n_y, rows, 256), jnp.bfloat16),
        in_specs=[SMEM] + [VMEM] * 5,
        out_specs=VMEM,
        scratch_shapes=[pltpu.VMEM((depth, n_keys), jnp.bfloat16)],
        compiler_params=pltpu.CompilerParams(vmem_limit_bytes=36 * MIB),
        name="attend",
    )(place, query, mine, other, value_up_s, value_up_l)


def merge_kernel(parts, out_s, out_l, out):
    n = parts.shape[0]

    def merged(first, width, stat):
        def stat_of(i, k):
            at = 192 + stat + 3 * k
            return (
                parts[i, :, at : at + 1].astype(jnp.float32)
                + parts[i, :, at + 1 : at + 2].astype(jnp.float32)
            ) + parts[i, :, at + 2 : at + 3].astype(jnp.float32)

        tops = [stat_of(i, 0) for i in range(n)]
        top = tops[0]
        for t in tops[1:]:
            top = jnp.maximum(top, t)
        shares = [stat_of(i, 1) * jnp.exp(tops[i] - top) for i in range(n)]
        total = sum(shares[1:], shares[0])
        acc = 0.0
        for i in range(n):
            acc = acc + parts[i, :, first : first + width].astype(jnp.float32) * (shares[i] / total)
        return acc.astype(jnp.bfloat16)

    large = merged(0, 128, 0)
    small = merged(128, 64, 6)
    mixed = jnp.dot(small, out_s[...], preferred_element_type=jnp.float32) + jnp.dot(
        large, out_l[...], preferred_element_type=jnp.float32
    )
    out[...] = mixed.astype(jnp.bfloat16)


def merge(parts, out_s, out_l):
    return pl.pallas_call(
        merge_kernel,
        out_shape=jax.ShapeDtypeStruct((parts.shape[1], out_s.shape[1]), jnp.bfloat16),
        in_specs=[VMEM] * 3,
        out_specs=VMEM,
        compiler_params=pltpu.CompilerParams(vmem_limit_bytes=8 * MIB),
        name="merge",
    )(parts, out_s, out_l)


def fetch_kernel(weights, out, arrived):
    copy = pltpu.make_async_copy(weights, out, arrived)
    copy.start()
    copy.wait()


def fetch(weights):
    return pl.pallas_call(
        fetch_kernel,
        out_shape=jax.ShapeDtypeStruct(weights.shape, weights.dtype),
        in_specs=[pl.BlockSpec(memory_space=pltpu.HBM)],
        out_specs=VMEM,
        scratch_shapes=[pltpu.SemaphoreType.DMA],
        compiler_params=pltpu.CompilerParams(vmem_limit_bytes=46 * MIB),
        name="fetch",
    )(weights)


def mixer_kernel(rows, weights, out):
    room = weights.shape[1] // 3
    both = jnp.dot(rows[...], weights[:, 0 : 2 * room], preferred_element_type=jnp.float32)
    gate = both[:, :room]
    hidden = (gate / (1.0 + jnp.exp(-gate)) * both[:, room:]).astype(jnp.bfloat16)
    part = lax.dot_general(hidden, weights[:, 2 * room :], NT, preferred_element_type=jnp.float32)
    out[...] = part.astype(out.dtype)


def mixer(rows, weights, dtype):
    return pl.pallas_call(
        mixer_kernel,
        out_shape=jax.ShapeDtypeStruct(rows.shape, dtype),
        in_specs=[VMEM] * 2,
        out_specs=VMEM,
        compiler_params=pltpu.CompilerParams(vmem_limit_bytes=16 * MIB),
    )(rows, weights)


def shards(
    residual,
    query_small,
    query_large,
    latent,
    rope_key,
    key_up_small,
    value_up_small,
    key_up_large,
    value_up_large,
    out_small,
    out_large,
    norm_gain,
    gate_weight,
    up_weight,
    down_weight,
):
    n_y = lax.axis_size(("yh", "yl"))
    z = lax.axis_index("z")
    y = lax.axis_index(("yh", "yl"))
    x = lax.axis_index("x")
    c = lax.axis_index("c")
    row_count = query_small.shape[0]
    rows, d = residual.shape
    place = (((z * n_y + y) * lax.axis_size("x") + x) * 2 + c).astype(jnp.int32).reshape(1)

    chunks = pack_weights(gate_weight, up_weight, down_weight, n_y)
    over_y = exchanged(chunks, ("yh", "yl"))
    weights = lax.all_gather(
        over_y.reshape(-1, over_y.shape[2]), "z", axis=0, tiled=True
    )

    positions = (z * n_y + y) * row_count + jnp.arange(row_count, dtype=jnp.int32)
    inverse = 1.0 / rope_base ** (jnp.arange(0, ROPE, 2, dtype=jnp.float32) / ROPE)
    angles = positions.astype(jnp.float32)[None, :] * inverse[:, None]
    query, packed = prepare(
        place,
        query_small.T,
        query_large.T,
        latent,
        rope_key.T,
        jnp.cos(angles),
        jnp.sin(angles),
        lax.axis_size("z"),
    )
    along_z = exchanged(packed, "z")
    queries = [query] + [
        lax.ppermute(query, ("yh", "yl"), [(i, (i + k) % n_y) for i in range(n_y)])
        for k in range(1, n_y)
    ]
    full = absorb(place, join(place, queries), key_up_small.T, key_up_large)
    mine = from_everyone(along_z, "x")
    other = partner(mine)

    partial = attention(place, full, mine, other, value_up_small.T, value_up_large)
    parts = exchanged(partial, ("yh", "yl"))
    mixed_part = merge(parts, out_small, out_large)
    tiles = exchanged(mixed_part.reshape(row_count // rows, rows, d), ("x", "c"))
    mixed = jnp.sum(tiles.astype(jnp.float32), axis=0).astype(jnp.bfloat16)
    stream = (residual.astype(jnp.float32) + mixed.astype(jnp.float32)).astype(jnp.bfloat16)
    as_float = stream.astype(jnp.float32)
    normed = as_float * lax.rsqrt(jnp.mean(as_float * as_float, axis=-1, keepdims=True) + norm_eps)
    normed = (normed * norm_gain.astype(jnp.float32)[None, :]).astype(jnp.bfloat16)

    here = from_everyone(normed, ("yl", "x")).reshape(-1, d)
    here, weights = lax.optimization_barrier((here, weights))
    there = partner(here)
    held = fetch(weights)
    part_there = mixer(there, held, jnp.bfloat16)
    sent = partner(part_there)
    part_here = mixer(here, held, jnp.float32)
    both = (part_here + sent.astype(jnp.float32)).astype(jnp.bfloat16)
    pieces = exchanged(both.reshape(-1, rows, d), ("yl", "x"))
    channel = jnp.sum(pieces.astype(jnp.float32), axis=0).astype(jnp.bfloat16)
    return (as_float + 0.5 * channel.astype(jnp.float32)).astype(jnp.bfloat16)


def solution(mesh):
    fine = Mesh(mesh.devices.reshape(-1, 2, 2, 4, 2), ("z", "yh", "yl", "x", "c"))
    sp = ("z", "yh", "yl")
    tp = ("x", "c")
    both = sp + tp
    placed = (
        P(both, None),
        P(sp, tp),
        P(sp, tp),
        P(sp, None),
        P(sp, None),
        P(None, tp),
        P(None, tp),
        P(None, tp),
        P(None, tp),
        P(tp, None),
        P(tp, None),
        P(),
        P(sp, tp),
        P(sp, tp),
        P(sp, tp),
    )
    return jax.shard_map(
        shards, mesh=fine, in_specs=placed, out_specs=P(both, None), check_vma=False
    )
```

```python
import jax
import jax.numpy as jnp
from jax import lax
from jax.experimental import pallas as pl
from jax.experimental.pallas import tpu as pltpu
from jax.sharding import Mesh
from jax.sharding import PartitionSpec as P


HEAD_SMALL = 64
HEAD_LARGE = 128
ROPE = 32
SCALE_SMALL = (HEAD_SMALL + ROPE) ** (-0.5)
SCALE_LARGE = (HEAD_LARGE + ROPE) ** (-0.5)

big_negative = -1e30
rope_base = 500000.0
norm_eps = 1e-06

NT = (((1,), (1,)), ((), ()))
MIB = 1024 * 1024
VMEM = pl.BlockSpec(memory_space=pltpu.VMEM)
SMEM = pl.BlockSpec(memory_space=pltpu.SMEM)


def where_in(place):
    core = lax.rem(place, 2)
    x = lax.rem(lax.div(place, 2), 4)
    y = lax.rem(lax.div(place, 8), 4)
    return lax.div(place, 32), y, x, core


def from_everyone(shard, axis):
    copies = jnp.broadcast_to(shard, (lax.axis_size(axis), *shard.shape))
    return lax.all_to_all(copies, axis, split_axis=0, concat_axis=0, tiled=True)


def exchanged(chunks, axis):
    return lax.all_to_all(chunks, axis, split_axis=0, concat_axis=0, tiled=True)


def partner(x):
    return lax.ppermute(x, "c", [(0, 1), (1, 0)])


def three_parts(v):
    high = v.astype(jnp.bfloat16).astype(jnp.float32)
    rest = v - high
    middle = rest.astype(jnp.bfloat16).astype(jnp.float32)
    low = (rest - middle).astype(jnp.bfloat16).astype(jnp.float32)
    return [high, middle, low]


def weights_kernel(gate, up, down, out):
    cut = gate.shape[1] // 2
    room = out.shape[2] // 3
    depth = gate.shape[0]
    blank = jnp.zeros((depth, room - cut), jnp.float32)
    for k, w in enumerate((gate, up, down)):
        whole = w[...].astype(jnp.float32)
        for j in range(2):
            half = jnp.concatenate([whole[:, cut * j : cut * (j + 1)], blank], axis=1)
            half = half.astype(jnp.bfloat16)
            for i in range(out.shape[0] // 2):
                out[2 * i + j, :, room * k : room * (k + 1)] = half


def pack_weights(gate, up, down, n_y):
    room = -(-(gate.shape[1] // 2) // 128) * 128
    return pl.pallas_call(
        weights_kernel,
        out_shape=jax.ShapeDtypeStruct((n_y, gate.shape[0], 3 * room), jnp.bfloat16),
        in_specs=[VMEM] * 3,
        out_specs=VMEM,
        name="pack_weights",
    )(gate, up, down)


def prepare_kernel(place, small, large, latent, rope_key, cosine_of, sine_of, query, packed, tall):
    _, _, x, core = where_in(place[0])
    half = ROPE // 2
    cosine = cosine_of[...]
    sine = sine_of[...]

    def turn(v):
        v = v.astype(jnp.float32)
        leading = v[0:half, :]
        trailing = v[half:, :]
        return jnp.concatenate(
            [leading * cosine - trailing * sine, trailing * cosine + leading * sine], axis=0
        )

    tall[0:256, :] = latent[...].astype(jnp.float32).T
    tall[256 : 256 + ROPE, :] = turn(rope_key[...])
    mine = tall[pl.ds(pl.multiple_of(64 * x + 32 * core, 32), 32), :]
    ours = tall[pl.ds(pl.multiple_of(256 + 8 * x, 8), 8), :]
    piece = jnp.concatenate([mine, ours], axis=0).astype(jnp.bfloat16)
    for k in range(packed.shape[0]):
        packed[k] = piece
    upright = jnp.concatenate(
        [
            large[0:HEAD_LARGE, :].astype(jnp.float32),
            small[0:HEAD_SMALL, :].astype(jnp.float32),
            turn(small[HEAD_SMALL:, :]) * SCALE_SMALL,
            turn(large[HEAD_LARGE:, :]) * SCALE_LARGE,
        ],
        axis=0,
    )
    query[...] = upright.T.astype(jnp.bfloat16)


def prepare(place, small, large, latent, rope_key, cosine, sine, n_z):
    rows = latent.shape[0]
    return pl.pallas_call(
        prepare_kernel,
        out_shape=(
            jax.ShapeDtypeStruct((rows, 256), jnp.bfloat16),
            jax.ShapeDtypeStruct((n_z, 40, rows), jnp.bfloat16),
        ),
        in_specs=[SMEM] + [VMEM] * 6,
        out_specs=(VMEM, VMEM),
        scratch_shapes=[pltpu.VMEM((256 + ROPE, rows), jnp.float32)],
        name="prepare",
    )(place, small, large, latent, rope_key, cosine, sine)


def join_kernel(place, *refs):
    *queries, out = refs
    n_y = len(queries)
    _, y, _, _ = where_in(place[0])
    for k, query in enumerate(queries):
        out[lax.rem(y - k + n_y, n_y)] = query[...]


def join(place, queries):
    return pl.pallas_call(
        join_kernel,
        out_shape=jax.ShapeDtypeStruct((len(queries), *queries[0].shape), jnp.bfloat16),
        in_specs=[SMEM] + [VMEM] * len(queries),
        out_specs=VMEM,
        compiler_params=pltpu.CompilerParams(vmem_limit_bytes=4 * MIB),
        name="join",
    )(place, *queries)


def absorb_kernel(place, query, key_up_s, key_up_l, out):
    n_y = query.shape[0]
    _, y, _, _ = where_in(place[0])
    row = lax.broadcasted_iota(jnp.int32, (128, 128), 0)
    lane = lax.broadcasted_iota(jnp.int32, (128, 128), 1)
    diagonal = jnp.where(row == lane, 1.0, 0.0)
    pick_lane = lax.broadcasted_iota(jnp.int32, (128, 96), 1)
    key_up_large = key_up_l[...].T
    for j in range(n_y):
        q = query[j]
        own = jnp.where(y == j, diagonal, 0.0)
        pick = jnp.where(pick_lane == j, 1.0, 0.0)
        heads = (
            (q[:, 0:128], q[:, 224:256], key_up_large, SCALE_LARGE),
            (q[:, 128:192], q[:, 192:224], key_up_s[...], SCALE_SMALL),
        )
        for h, (nope, rope, key_up, scale) in enumerate(heads):
            wide = jnp.dot(nope, key_up, preferred_element_type=jnp.float32)
            tail = jnp.concatenate([rope.astype(jnp.float32), pick], axis=1)
            whole = jnp.concatenate([wide * scale, tail, own], axis=1)
            out[j, h, :, :] = whole.astype(jnp.bfloat16)


def absorb(place, query, key_up_s, key_up_l):
    n_y, rows = query.shape[:2]
    return pl.pallas_call(
        absorb_kernel,
        out_shape=jax.ShapeDtypeStruct((n_y, 2, rows, 512), jnp.bfloat16),
        in_specs=[SMEM] + [VMEM] * 3,
        out_specs=VMEM,
        compiler_params=pltpu.CompilerParams(vmem_limit_bytes=8 * MIB),
        name="absorb",
    )(place, query, key_up_s, key_up_l)


def attention_kernel(place, query, mine, other, value_up_s, value_up_l, out, keys):
    z, y, _, c = where_in(place[0])
    n_x, n_z = mine.shape[0], mine.shape[1]
    n_y = query.shape[0]
    row = lax.broadcasted_iota(jnp.int32, (128, 128), 0)
    lane = lax.broadcasted_iota(jnp.int32, (128, 128), 1)
    for k in range(n_z):
        lanes = pl.ds(128 * k, 128)
        for x in range(n_x):
            here = pl.multiple_of(64 * x + 32 * c, 32)
            there = pl.multiple_of(64 * x + 32 * (1 - c), 32)
            keys[pl.ds(here, 32), lanes] = mine[x, k, 0:32, :]
            keys[pl.ds(there, 32), lanes] = other[x, k, 0:32, :]
        ropes = [mine[x, k, 32:40, :].astype(jnp.float32) for x in range(n_x)]
        keys[256 : 256 + ROPE, lanes] = jnp.concatenate(ropes, axis=0).astype(jnp.bfloat16)
        hidden_from = (k > z) | ((k == z) & (y > row))
        bias = jnp.where(hidden_from & (row < n_y), big_negative, 0.0)
        keys[288:384, lanes] = bias[0:96, :].astype(jnp.bfloat16)
        later = jnp.where((lane > row) & (k == z), big_negative, 0.0)
        keys[384:512, lanes] = later.astype(jnp.bfloat16)
    stat_lane = lax.broadcasted_iota(jnp.int32, (128, 64), 1)

    full = query[...].reshape(n_y * 256, query.shape[3])
    score = jnp.dot(full, keys[...], preferred_element_type=jnp.float32)
    tops = jnp.max(score, axis=1, keepdims=True)
    weight = jnp.exp(score - tops)
    totals = jnp.sum(weight, axis=1, keepdims=True)
    summed = lax.dot_general(
        weight.astype(jnp.bfloat16), keys[0:256, :], NT, preferred_element_type=jnp.float32
    )
    summed = (summed / totals).astype(jnp.bfloat16)
    for j in range(n_y):
        large = slice(256 * j, 256 * j + 128)
        small = slice(256 * j + 128, 256 * j + 256)
        value_l = jnp.dot(summed[large], value_up_l[...], preferred_element_type=jnp.float32)
        value_s = lax.dot_general(
            summed[small], value_up_s[...], NT, preferred_element_type=jnp.float32
        )
        stats = jnp.zeros((128, 64), jnp.float32)
        parts = [
            p for v in (tops[large], totals[large], tops[small], totals[small]) for p in three_parts(v)
        ]
        for i, part in enumerate(parts):
            stats = jnp.where(stat_lane == i, part, stats)
        out[j, :, 0:128] = value_l.astype(jnp.bfloat16)
        out[j, :, 128:256] = jnp.concatenate([value_s, stats], axis=1).astype(jnp.bfloat16)


def attention(place, query, mine, other, value_up_s, value_up_l):
    n_y, _, rows, depth = query.shape
    n_keys = 128 * mine.shape[1]
    return pl.pallas_call(
        attention_kernel,
        out_shape=jax.ShapeDtypeStruct((n_y, rows, 256), jnp.bfloat16),
        in_specs=[SMEM] + [VMEM] * 5,
        out_specs=VMEM,
        scratch_shapes=[pltpu.VMEM((depth, n_keys), jnp.bfloat16)],
        compiler_params=pltpu.CompilerParams(vmem_limit_bytes=36 * MIB),
        name="attend",
    )(place, query, mine, other, value_up_s, value_up_l)


def stack_kernel(out_l, out_s, out):
    rows = out_l.shape[0]
    out[0:rows, :] = out_l[...]
    out[rows:, :] = out_s[...]


def stack(out_l, out_s):
    rows = out_l.shape[0] + out_s.shape[0]
    return pl.pallas_call(
        stack_kernel,
        out_shape=jax.ShapeDtypeStruct((rows, out_l.shape[1]), jnp.bfloat16),
        in_specs=[VMEM] * 2,
        out_specs=VMEM,
        name="stack_out",
    )(out_l, out_s)


def halves_kernel(before, after, large, small):
    large[...] = before[0:HEAD_LARGE, :]
    small[...] = after[HEAD_LARGE:, :]


def halves(before, after):
    d = before.shape[1]
    return pl.pallas_call(
        halves_kernel,
        out_shape=(
            jax.ShapeDtypeStruct((HEAD_LARGE, d), jnp.bfloat16),
            jax.ShapeDtypeStruct((HEAD_SMALL, d), jnp.bfloat16),
        ),
        in_specs=[VMEM] * 2,
        out_specs=(VMEM, VMEM),
        compiler_params=pltpu.CompilerParams(vmem_limit_bytes=8 * MIB),
        name="halves",
    )(before, after)


def merge_kernel(place, parts, own, before, after, far_l, far_s, mine, theirs):
    _, _, x, core = where_in(place[0])
    n_x = 4
    n_y = parts.shape[0] // n_x
    rows = mine.shape[0]

    def attended(k):
        column = lax.rem(x - k + n_x, n_x)
        pieces = [parts[n_x * i + column].astype(jnp.float32) for i in range(n_y)]

        def merged(first, width, stat):
            def stat_of(piece, which):
                at = 192 + stat + 3 * which
                return (piece[:, at : at + 1] + piece[:, at + 1 : at + 2]) + piece[:, at + 2 : at + 3]

            tops = [stat_of(piece, 0) for piece in pieces]
            top = tops[0]
            for t in tops[1:]:
                top = jnp.maximum(top, t)
            shares = [stat_of(p, 1) * jnp.exp(t - top) for p, t in zip(pieces, tops)]
            total = sum(shares[1:], shares[0])
            acc = 0.0
            for piece, share in zip(pieces, shares):
                acc = acc + piece[:, first : first + width] * (share / total)
            return acc.astype(jnp.bfloat16)

        return merged(0, HEAD_LARGE, 0), merged(HEAD_LARGE, HEAD_SMALL, 6)

    total = None
    for k, (large_w, small_w) in enumerate(
        (
            (own[0:HEAD_LARGE, :], own[HEAD_LARGE:, :]),
            (before[0:HEAD_LARGE, :], before[HEAD_LARGE:, :]),
            (far_l[...], far_s[...]),
            (after[0:HEAD_LARGE, :], after[HEAD_LARGE:, :]),
        )
    ):
        large, small = attended(k)
        term = jnp.dot(large, large_w, preferred_element_type=jnp.float32) + jnp.dot(
            small, small_w, preferred_element_type=jnp.float32
        )
        total = term if total is None else total + term
    top, bottom = total[0:rows, :], total[rows : 2 * rows, :]
    mine[...] = jnp.where(core == 0, top, bottom)
    theirs[...] = jnp.where(core == 0, bottom, top).astype(jnp.bfloat16)


def merge(place, parts, own, before, after, far_l, far_s):
    rows, d = parts.shape[1] // 2, own.shape[1]
    return pl.pallas_call(
        merge_kernel,
        out_shape=(
            jax.ShapeDtypeStruct((rows, d), jnp.float32),
            jax.ShapeDtypeStruct((rows, d), jnp.bfloat16),
        ),
        in_specs=[SMEM] + [VMEM] * 6,
        out_specs=(VMEM, VMEM),
        compiler_params=pltpu.CompilerParams(vmem_limit_bytes=16 * MIB),
        name="merge",
    )(place, parts, own, before, after, far_l, far_s)


def norm_kernel(mine, sent, residual, gain, copies, stream):
    mixed = (mine[...] + sent[...].astype(jnp.float32)).astype(jnp.bfloat16).astype(jnp.float32)
    total = (residual[...].astype(jnp.float32) + mixed).astype(jnp.bfloat16)
    stream[...] = total
    wide = total.astype(jnp.float32)
    normed = wide * lax.rsqrt(jnp.mean(wide * wide, axis=-1, keepdims=True) + norm_eps)
    normed = (normed * gain[...].astype(jnp.float32)).astype(jnp.bfloat16)
    for k in range(copies.shape[0]):
        copies[k] = normed


def norm(mine, sent, residual, gain, count):
    return pl.pallas_call(
        norm_kernel,
        out_shape=(
            jax.ShapeDtypeStruct((count, *residual.shape), jnp.bfloat16),
            jax.ShapeDtypeStruct(residual.shape, jnp.bfloat16),
        ),
        in_specs=[VMEM] * 4,
        out_specs=(VMEM, VMEM),
        compiler_params=pltpu.CompilerParams(vmem_limit_bytes=8 * MIB),
        name="norm",
    )(mine, sent, residual, gain)


def fetch_kernel(weights, out, arrived):
    copy = pltpu.make_async_copy(weights, out, arrived)
    copy.start()
    copy.wait()


def fetch(weights):
    return pl.pallas_call(
        fetch_kernel,
        out_shape=jax.ShapeDtypeStruct(weights.shape, weights.dtype),
        in_specs=[pl.BlockSpec(memory_space=pltpu.HBM)],
        out_specs=VMEM,
        scratch_shapes=[pltpu.SemaphoreType.DMA],
        compiler_params=pltpu.CompilerParams(vmem_limit_bytes=46 * MIB),
        name="fetch",
    )(weights)


def mixer_kernel(rows, weights, out):
    room = weights.shape[1] // 3
    both = jnp.dot(rows[...], weights[:, 0 : 2 * room], preferred_element_type=jnp.float32)
    gate = both[:, :room]
    hidden = (gate / (1.0 + jnp.exp(-gate)) * both[:, room:]).astype(jnp.bfloat16)
    part = lax.dot_general(hidden, weights[:, 2 * room :], NT, preferred_element_type=jnp.float32)
    out[...] = part.astype(out.dtype)


def mixer(rows, weights, dtype):
    return pl.pallas_call(
        mixer_kernel,
        out_shape=jax.ShapeDtypeStruct(rows.shape, dtype),
        in_specs=[VMEM] * 2,
        out_specs=VMEM,
        compiler_params=pltpu.CompilerParams(vmem_limit_bytes=16 * MIB),
    )(rows, weights)


def shards(
    residual,
    query_small,
    query_large,
    latent,
    rope_key,
    key_up_small,
    value_up_small,
    key_up_large,
    value_up_large,
    out_small,
    out_large,
    norm_gain,
    gate_weight,
    up_weight,
    down_weight,
):
    n_y = lax.axis_size(("yh", "yl"))
    n_x = lax.axis_size("x")
    z = lax.axis_index("z")
    y = lax.axis_index(("yh", "yl"))
    x = lax.axis_index("x")
    c = lax.axis_index("c")
    row_count = query_small.shape[0]
    rows, d = residual.shape
    place = (((z * n_y + y) * lax.axis_size("x") + x) * 2 + c).astype(jnp.int32).reshape(1)

    chunks = pack_weights(gate_weight, up_weight, down_weight, n_y)
    over_y = exchanged(chunks, ("yh", "yl"))
    weights = lax.all_gather(
        over_y.reshape(-1, over_y.shape[2]), "z", axis=0, tiled=True
    )

    own_out = stack(out_large, out_small)
    before = lax.ppermute(own_out, "x", [(i, (i + 1) % n_x) for i in range(n_x)])
    after = lax.ppermute(own_out, "x", [(i, (i - 1) % n_x) for i in range(n_x)])
    pass_l, pass_s = halves(before, after)
    far_l = lax.ppermute(pass_l, "x", [(i, (i + 1) % n_x) for i in range(n_x)])
    far_s = lax.ppermute(pass_s, "x", [(i, (i - 1) % n_x) for i in range(n_x)])

    positions = (z * n_y + y) * row_count + jnp.arange(row_count, dtype=jnp.int32)
    inverse = 1.0 / rope_base ** (jnp.arange(0, ROPE, 2, dtype=jnp.float32) / ROPE)
    angles = positions.astype(jnp.float32)[None, :] * inverse[:, None]
    query, packed = prepare(
        place,
        query_small.T,
        query_large.T,
        latent,
        rope_key.T,
        jnp.cos(angles),
        jnp.sin(angles),
        lax.axis_size("z"),
    )
    along_z = exchanged(packed, "z")
    queries = [query] + [
        lax.ppermute(query, ("yh", "yl"), [(i, (i + k) % n_y) for i in range(n_y)])
        for k in range(1, n_y)
    ]
    full = absorb(place, join(place, queries), key_up_small.T, key_up_large)
    mine = from_everyone(along_z, "x")
    other = partner(mine)

    partial = attention(place, full, mine, other, value_up_small.T, value_up_large)
    parts = exchanged(
        partial.reshape(n_y * n_x, row_count // n_x, partial.shape[2]), ("yh", "yl", "x")
    )
    mine_part, theirs_part = merge(place, parts, own_out, before, after, far_l, far_s)
    sent_part = partner(theirs_part)
    copies, stream = norm(
        mine_part, sent_part, residual, norm_gain.reshape(1, d), lax.axis_size(("yl", "x"))
    )
    as_float = stream.astype(jnp.float32)
    here = exchanged(copies, ("yl", "x")).reshape(-1, d)
    here, weights = lax.optimization_barrier((here, weights))
    there = partner(here)
    held = fetch(weights)
    part_there = mixer(there, held, jnp.bfloat16)
    sent = partner(part_there)
    part_here = mixer(here, held, jnp.float32)
    both = (part_here + sent.astype(jnp.float32)).astype(jnp.bfloat16)
    pieces = exchanged(both.reshape(-1, rows, d), ("yl", "x"))
    channel = jnp.sum(pieces.astype(jnp.float32), axis=0).astype(jnp.bfloat16)
    return (as_float + 0.5 * channel.astype(jnp.float32)).astype(jnp.bfloat16)


def solution(mesh):
    fine = Mesh(mesh.devices.reshape(-1, 2, 2, 4, 2), ("z", "yh", "yl", "x", "c"))
    sp = ("z", "yh", "yl")
    tp = ("x", "c")
    both = sp + tp
    placed = (
        P(both, None),
        P(sp, tp),
        P(sp, tp),
        P(sp, None),
        P(sp, None),
        P(None, tp),
        P(None, tp),
        P(None, tp),
        P(None, tp),
        P(tp, None),
        P(tp, None),
        P(),
        P(sp, tp),
        P(sp, tp),
        P(sp, tp),
    )
    return jax.shard_map(
        shards, mesh=fine, in_specs=placed, out_specs=P(both, None), check_vma=False
    )
```

```python
import jax
import jax.numpy as jnp
from jax import lax
from jax.experimental import pallas as pl
from jax.experimental.pallas import tpu as pltpu
from jax.sharding import Mesh
from jax.sharding import PartitionSpec as P


HEAD_SMALL = 64
HEAD_LARGE = 128
ROPE = 32
SCALE_SMALL = (HEAD_SMALL + ROPE) ** (-0.5)
SCALE_LARGE = (HEAD_LARGE + ROPE) ** (-0.5)

big_negative = -1e30
rope_base = 500000.0
norm_eps = 1e-06

NT = (((1,), (1,)), ((), ()))
MIB = 1024 * 1024
VMEM = pl.BlockSpec(memory_space=pltpu.VMEM)
SMEM = pl.BlockSpec(memory_space=pltpu.SMEM)


def where_in(place):
    core = lax.rem(place, 2)
    x = lax.rem(lax.div(place, 2), 4)
    y = lax.rem(lax.div(place, 8), 4)
    return lax.div(place, 32), y, x, core


def from_everyone(shard, axis):
    copies = jnp.broadcast_to(shard, (lax.axis_size(axis), *shard.shape))
    return lax.all_to_all(copies, axis, split_axis=0, concat_axis=0, tiled=True)


def exchanged(chunks, axis):
    return lax.all_to_all(chunks, axis, split_axis=0, concat_axis=0, tiled=True)


def partner(x):
    return lax.ppermute(x, "c", [(0, 1), (1, 0)])


def three_parts(v):
    high = v.astype(jnp.bfloat16).astype(jnp.float32)
    rest = v - high
    middle = rest.astype(jnp.bfloat16).astype(jnp.float32)
    low = (rest - middle).astype(jnp.bfloat16).astype(jnp.float32)
    return [high, middle, low]


def weights_kernel(gate, up, down, out):
    cut = gate.shape[1] // 2
    room = out.shape[2] // 3
    depth = gate.shape[0]
    blank = jnp.zeros((depth, room - cut), jnp.float32)
    for k, w in enumerate((gate, up, down)):
        whole = w[...].astype(jnp.float32)
        for j in range(2):
            half = jnp.concatenate([whole[:, cut * j : cut * (j + 1)], blank], axis=1)
            half = half.astype(jnp.bfloat16)
            for i in range(out.shape[0] // 2):
                out[2 * i + j, :, room * k : room * (k + 1)] = half


def pack_weights(gate, up, down, n_y):
    room = -(-(gate.shape[1] // 2) // 128) * 128
    return pl.pallas_call(
        weights_kernel,
        out_shape=jax.ShapeDtypeStruct((n_y, gate.shape[0], 3 * room), jnp.bfloat16),
        in_specs=[VMEM] * 3,
        out_specs=VMEM,
        name="pack_weights",
    )(gate, up, down)


def prepare_kernel(place, small, large, latent, rope_key, cosine_of, sine_of, query, packed, tall):
    _, _, x, core = where_in(place[0])
    half = ROPE // 2
    cosine = cosine_of[...]
    sine = sine_of[...]

    def turn(v):
        v = v.astype(jnp.float32)
        leading = v[0:half, :]
        trailing = v[half:, :]
        return jnp.concatenate(
            [leading * cosine - trailing * sine, trailing * cosine + leading * sine], axis=0
        )

    tall[0:256, :] = latent[...].astype(jnp.float32).T
    tall[256 : 256 + ROPE, :] = turn(rope_key[...])
    mine = tall[pl.ds(pl.multiple_of(64 * x + 32 * core, 32), 32), :]
    ours = tall[pl.ds(pl.multiple_of(256 + 8 * x, 8), 8), :]
    piece = jnp.concatenate([mine, ours], axis=0).astype(jnp.bfloat16)
    for k in range(packed.shape[0]):
        packed[k] = piece
    upright = jnp.concatenate(
        [
            large[0:HEAD_LARGE, :].astype(jnp.float32),
            small[0:HEAD_SMALL, :].astype(jnp.float32),
            turn(small[HEAD_SMALL:, :]) * SCALE_SMALL,
            turn(large[HEAD_LARGE:, :]) * SCALE_LARGE,
        ],
        axis=0,
    )
    query[...] = upright.T.astype(jnp.bfloat16)


def prepare(place, small, large, latent, rope_key, cosine, sine, n_z):
    rows = latent.shape[0]
    return pl.pallas_call(
        prepare_kernel,
        out_shape=(
            jax.ShapeDtypeStruct((rows, 256), jnp.bfloat16),
            jax.ShapeDtypeStruct((n_z, 40, rows), jnp.bfloat16),
        ),
        in_specs=[SMEM] + [VMEM] * 6,
        out_specs=(VMEM, VMEM),
        scratch_shapes=[pltpu.VMEM((256 + ROPE, rows), jnp.float32)],
        compiler_params=pltpu.CompilerParams(vmem_limit_bytes=4 * MIB),
        name="prepare",
    )(place, small, large, latent, rope_key, cosine, sine)


def join_kernel(place, *refs):
    *queries, out = refs
    n_y = len(queries)
    _, y, _, _ = where_in(place[0])
    for k, query in enumerate(queries):
        out[lax.rem(y - k + n_y, n_y)] = query[...]


def join(place, queries):
    return pl.pallas_call(
        join_kernel,
        out_shape=jax.ShapeDtypeStruct((len(queries), *queries[0].shape), jnp.bfloat16),
        in_specs=[SMEM] + [VMEM] * len(queries),
        out_specs=VMEM,
        compiler_params=pltpu.CompilerParams(vmem_limit_bytes=4 * MIB),
        name="join",
    )(place, *queries)


def absorb_kernel(place, query, key_up_s, key_up_l, out):
    n_y = query.shape[0]
    _, y, _, _ = where_in(place[0])
    row = lax.broadcasted_iota(jnp.int32, (128, 128), 0)
    lane = lax.broadcasted_iota(jnp.int32, (128, 128), 1)
    diagonal = jnp.where(row == lane, 1.0, 0.0)
    pick_lane = lax.broadcasted_iota(jnp.int32, (128, 96), 1)
    key_up_large = key_up_l[...].T
    for j in range(n_y):
        q = query[j]
        own = jnp.where(y == j, diagonal, 0.0)
        pick = jnp.where(pick_lane == j, 1.0, 0.0)
        heads = (
            (q[:, 0:128], q[:, 224:256], key_up_large, SCALE_LARGE),
            (q[:, 128:192], q[:, 192:224], key_up_s[...], SCALE_SMALL),
        )
        for h, (nope, rope, key_up, scale) in enumerate(heads):
            wide = jnp.dot(nope, key_up, preferred_element_type=jnp.float32)
            tail = jnp.concatenate([rope.astype(jnp.float32), pick], axis=1)
            whole = jnp.concatenate([wide * scale, tail, own], axis=1)
            out[j, h, :, :] = whole.astype(jnp.bfloat16)


def absorb(place, query, key_up_s, key_up_l):
    n_y, rows = query.shape[:2]
    return pl.pallas_call(
        absorb_kernel,
        out_shape=jax.ShapeDtypeStruct((n_y, 2, rows, 512), jnp.bfloat16),
        in_specs=[SMEM] + [VMEM] * 3,
        out_specs=VMEM,
        compiler_params=pltpu.CompilerParams(vmem_limit_bytes=8 * MIB),
        name="absorb",
    )(place, query, key_up_s, key_up_l)


def attention_kernel(place, query, mine, other, value_up_s, value_up_l, out, keys):
    z, y, _, c = where_in(place[0])
    n_x, n_z = mine.shape[0], mine.shape[1]
    n_y = query.shape[0]
    row = lax.broadcasted_iota(jnp.int32, (128, 128), 0)
    lane = lax.broadcasted_iota(jnp.int32, (128, 128), 1)
    for k in range(n_z):
        lanes = pl.ds(128 * k, 128)
        for x in range(n_x):
            here = pl.multiple_of(64 * x + 32 * c, 32)
            there = pl.multiple_of(64 * x + 32 * (1 - c), 32)
            keys[pl.ds(here, 32), lanes] = mine[x, k, 0:32, :]
            keys[pl.ds(there, 32), lanes] = other[x, k, 0:32, :]
        ropes = [mine[x, k, 32:40, :].astype(jnp.float32) for x in range(n_x)]
        keys[256 : 256 + ROPE, lanes] = jnp.concatenate(ropes, axis=0).astype(jnp.bfloat16)
        hidden_from = (k > z) | ((k == z) & (y > row))
        bias = jnp.where(hidden_from & (row < n_y), big_negative, 0.0)
        keys[288:384, lanes] = bias[0:96, :].astype(jnp.bfloat16)
        later = jnp.where((lane > row) & (k == z), big_negative, 0.0)
        keys[384:512, lanes] = later.astype(jnp.bfloat16)
    stat_lane = lax.broadcasted_iota(jnp.int32, (128, 64), 1)

    full = query[...].reshape(n_y * 256, query.shape[3])
    score = jnp.dot(full, keys[...], preferred_element_type=jnp.float32)
    tops = jnp.max(score, axis=1, keepdims=True)
    weight = jnp.exp(score - tops)
    totals = jnp.sum(weight, axis=1, keepdims=True)
    summed = lax.dot_general(
        weight.astype(jnp.bfloat16), keys[0:256, :], NT, preferred_element_type=jnp.float32
    )
    summed = (summed / totals).astype(jnp.bfloat16)
    for j in range(n_y):
        large = slice(256 * j, 256 * j + 128)
        small = slice(256 * j + 128, 256 * j + 256)
        value_l = jnp.dot(summed[large], value_up_l[...], preferred_element_type=jnp.float32)
        value_s = lax.dot_general(
            summed[small], value_up_s[...], NT, preferred_element_type=jnp.float32
        )
        stats = jnp.zeros((128, 64), jnp.float32)
        parts = [
            p for v in (tops[large], totals[large], tops[small], totals[small]) for p in three_parts(v)
        ]
        for i, part in enumerate(parts):
            stats = jnp.where(stat_lane == i, part, stats)
        whole = jnp.concatenate([value_l, jnp.concatenate([value_s, stats], axis=1)], axis=1)
        for core in range(2):
            picked = [whole[32 * x + 16 * core : 32 * x + 16 * core + 16] for x in range(n_x)]
            out[2 * j + core] = jnp.concatenate(picked, axis=0).astype(jnp.bfloat16)


def attention(place, query, mine, other, value_up_s, value_up_l):
    n_y, _, rows, depth = query.shape
    n_keys = 128 * mine.shape[1]
    return pl.pallas_call(
        attention_kernel,
        out_shape=jax.ShapeDtypeStruct((2 * n_y, rows // 2, 256), jnp.bfloat16),
        in_specs=[SMEM] + [VMEM] * 5,
        out_specs=VMEM,
        scratch_shapes=[pltpu.VMEM((depth, n_keys), jnp.bfloat16)],
        compiler_params=pltpu.CompilerParams(vmem_limit_bytes=36 * MIB),
        name="attend",
    )(place, query, mine, other, value_up_s, value_up_l)


def merge_kernel(place, parts, own_s, own_l, their_s, their_l, out):
    _, _, _, core = where_in(place[0])
    n_y = parts.shape[0] // 2

    def attended(column):
        pieces = [parts[2 * i + column].astype(jnp.float32) for i in range(n_y)]

        def merged(first, width, stat):
            def stat_of(piece, which):
                at = 192 + stat + 3 * which
                return (piece[:, at : at + 1] + piece[:, at + 1 : at + 2]) + piece[:, at + 2 : at + 3]

            tops = [stat_of(piece, 0) for piece in pieces]
            top = tops[0]
            for t in tops[1:]:
                top = jnp.maximum(top, t)
            shares = [stat_of(p, 1) * jnp.exp(t - top) for p, t in zip(pieces, tops)]
            total = sum(shares[1:], shares[0])
            acc = 0.0
            for piece, share in zip(pieces, shares):
                acc = acc + piece[:, first : first + width] * (share / total)
            return acc.astype(jnp.bfloat16)

        return merged(0, HEAD_LARGE, 0), merged(HEAD_LARGE, HEAD_SMALL, 6)

    total = None
    for column, small_w, large_w in ((core, own_s, own_l), (1 - core, their_s, their_l)):
        large, small = attended(column)
        term = jnp.dot(large, large_w[...], preferred_element_type=jnp.float32) + jnp.dot(
            small, small_w[...], preferred_element_type=jnp.float32
        )
        total = term if total is None else total + term
    out[...] = total.astype(jnp.bfloat16)


def merge(place, parts, own_s, own_l, their_s, their_l):
    return pl.pallas_call(
        merge_kernel,
        out_shape=jax.ShapeDtypeStruct((parts.shape[1], own_s.shape[1]), jnp.bfloat16),
        in_specs=[SMEM] + [VMEM] * 5,
        out_specs=VMEM,
        compiler_params=pltpu.CompilerParams(vmem_limit_bytes=8 * MIB),
        name="merge",
    )(place, parts, own_s, own_l, their_s, their_l)


def fetch_kernel(weights, out, arrived):
    copy = pltpu.make_async_copy(weights, out, arrived)
    copy.start()
    copy.wait()


def fetch(weights):
    return pl.pallas_call(
        fetch_kernel,
        out_shape=jax.ShapeDtypeStruct(weights.shape, weights.dtype),
        in_specs=[pl.BlockSpec(memory_space=pltpu.HBM)],
        out_specs=VMEM,
        scratch_shapes=[pltpu.SemaphoreType.DMA],
        compiler_params=pltpu.CompilerParams(vmem_limit_bytes=46 * MIB),
        name="fetch",
    )(weights)


def mixer_kernel(rows, weights, out):
    room = weights.shape[1] // 3
    both = jnp.dot(rows[...], weights[:, 0 : 2 * room], preferred_element_type=jnp.float32)
    gate = both[:, :room]
    hidden = (gate / (1.0 + jnp.exp(-gate)) * both[:, room:]).astype(jnp.bfloat16)
    part = lax.dot_general(hidden, weights[:, 2 * room :], NT, preferred_element_type=jnp.float32)
    out[...] = part.astype(out.dtype)


def mixer(rows, weights, dtype):
    return pl.pallas_call(
        mixer_kernel,
        out_shape=jax.ShapeDtypeStruct(rows.shape, dtype),
        in_specs=[VMEM] * 2,
        out_specs=VMEM,
        compiler_params=pltpu.CompilerParams(vmem_limit_bytes=16 * MIB),
    )(rows, weights)


def shards(
    residual,
    query_small,
    query_large,
    latent,
    rope_key,
    key_up_small,
    value_up_small,
    key_up_large,
    value_up_large,
    out_small,
    out_large,
    norm_gain,
    gate_weight,
    up_weight,
    down_weight,
):
    n_y = lax.axis_size(("yh", "yl"))
    z = lax.axis_index("z")
    y = lax.axis_index(("yh", "yl"))
    x = lax.axis_index("x")
    c = lax.axis_index("c")
    row_count = query_small.shape[0]
    rows, d = residual.shape
    place = (((z * n_y + y) * lax.axis_size("x") + x) * 2 + c).astype(jnp.int32).reshape(1)

    chunks = pack_weights(gate_weight, up_weight, down_weight, n_y)
    over_y = exchanged(chunks, ("yh", "yl"))
    weights = lax.all_gather(
        over_y.reshape(-1, over_y.shape[2]), "z", axis=0, tiled=True
    )

    their_small = partner(out_small)
    their_large = partner(out_large)

    positions = (z * n_y + y) * row_count + jnp.arange(row_count, dtype=jnp.int32)
    inverse = 1.0 / rope_base ** (jnp.arange(0, ROPE, 2, dtype=jnp.float32) / ROPE)
    angles = positions.astype(jnp.float32)[None, :] * inverse[:, None]
    query, packed = prepare(
        place,
        query_small.T,
        query_large.T,
        latent,
        rope_key.T,
        jnp.cos(angles),
        jnp.sin(angles),
        lax.axis_size("z"),
    )
    along_z = exchanged(packed, "z")
    queries = [query] + [
        lax.ppermute(query, ("yh", "yl"), [(i, (i + k) % n_y) for i in range(n_y)])
        for k in range(1, n_y)
    ]
    full = absorb(place, join(place, queries), key_up_small.T, key_up_large)
    mine = from_everyone(along_z, "x")
    other = partner(mine)

    partial = attention(place, full, mine, other, value_up_small.T, value_up_large)
    parts = exchanged(partial, ("yh", "yl", "c"))
    mixed_part = merge(place, parts, out_small, out_large, their_small, their_large)
    tiles = exchanged(mixed_part.reshape(-1, rows, d), "x")
    mixed = jnp.sum(tiles.astype(jnp.float32), axis=0).astype(jnp.bfloat16)
    stream = (residual.astype(jnp.float32) + mixed.astype(jnp.float32)).astype(jnp.bfloat16)
    as_float = stream.astype(jnp.float32)
    normed = as_float * lax.rsqrt(jnp.mean(as_float * as_float, axis=-1, keepdims=True) + norm_eps)
    normed = (normed * norm_gain.astype(jnp.float32)[None, :]).astype(jnp.bfloat16)

    here = from_everyone(normed, ("yl", "x")).reshape(-1, d)
    here, weights = lax.optimization_barrier((here, weights))
    there = partner(here)
    held = fetch(weights)
    part_there = mixer(there, held, jnp.bfloat16)
    sent = partner(part_there)
    part_here = mixer(here, held, jnp.float32)
    both = (part_here + sent.astype(jnp.float32)).astype(jnp.bfloat16)
    pieces = exchanged(both.reshape(-1, rows, d), ("yl", "x"))
    channel = jnp.sum(pieces.astype(jnp.float32), axis=0).astype(jnp.bfloat16)
    return (as_float + 0.5 * channel.astype(jnp.float32)).astype(jnp.bfloat16)


def solution(mesh):
    fine = Mesh(mesh.devices.reshape(-1, 2, 2, 4, 2), ("z", "yh", "yl", "x", "c"))
    sp = ("z", "yh", "yl")
    tp = ("x", "c")
    both = sp + tp
    placed = (
        P(both, None),
        P(sp, tp),
        P(sp, tp),
        P(sp, None),
        P(sp, None),
        P(None, tp),
        P(None, tp),
        P(None, tp),
        P(None, tp),
        P(tp, None),
        P(tp, None),
        P(),
        P(sp, tp),
        P(sp, tp),
        P(sp, tp),
    )
    return jax.shard_map(
        shards, mesh=fine, in_specs=placed, out_specs=P(both, None), check_vma=False
    )
```

```python
import jax
import jax.numpy as jnp
from jax import lax
from jax.experimental import pallas as pl
from jax.experimental.pallas import tpu as pltpu
from jax.sharding import Mesh
from jax.sharding import PartitionSpec as P


HEAD_SMALL = 64
HEAD_LARGE = 128
ROPE = 32
SCALE_SMALL = (HEAD_SMALL + ROPE) ** (-0.5)
SCALE_LARGE = (HEAD_LARGE + ROPE) ** (-0.5)

big_negative = -1e30
rope_base = 500000.0
norm_eps = 1e-06

NT = (((1,), (1,)), ((), ()))
MIB = 1024 * 1024
VMEM = pl.BlockSpec(memory_space=pltpu.VMEM)
SMEM = pl.BlockSpec(memory_space=pltpu.SMEM)


def where_in(place):
    core = lax.rem(place, 2)
    x = lax.rem(lax.div(place, 2), 4)
    y = lax.rem(lax.div(place, 8), 4)
    return lax.div(place, 32), y, x, core


def from_everyone(shard, axis):
    copies = jnp.broadcast_to(shard, (lax.axis_size(axis), *shard.shape))
    return lax.all_to_all(copies, axis, split_axis=0, concat_axis=0, tiled=True)


def exchanged(chunks, axis):
    return lax.all_to_all(chunks, axis, split_axis=0, concat_axis=0, tiled=True)


def partner(x):
    return lax.ppermute(x, "c", [(0, 1), (1, 0)])


def three_parts(v):
    high = v.astype(jnp.bfloat16).astype(jnp.float32)
    rest = v - high
    middle = rest.astype(jnp.bfloat16).astype(jnp.float32)
    low = (rest - middle).astype(jnp.bfloat16).astype(jnp.float32)
    return [high, middle, low]


def weights_kernel(gate, up, down, out):
    cut = gate.shape[1] // 2
    room = out.shape[2] // 3
    depth = gate.shape[0]
    blank = jnp.zeros((depth, room - cut), jnp.float32)
    for k, w in enumerate((gate, up, down)):
        whole = w[...].astype(jnp.float32)
        for j in range(2):
            half = jnp.concatenate([whole[:, cut * j : cut * (j + 1)], blank], axis=1)
            half = half.astype(jnp.bfloat16)
            for i in range(out.shape[0] // 2):
                out[2 * i + j, :, room * k : room * (k + 1)] = half


def pack_weights(gate, up, down, n_y):
    room = -(-(gate.shape[1] // 2) // 128) * 128
    return pl.pallas_call(
        weights_kernel,
        out_shape=jax.ShapeDtypeStruct((n_y, gate.shape[0], 3 * room), jnp.bfloat16),
        in_specs=[VMEM] * 3,
        out_specs=VMEM,
        name="pack_weights",
    )(gate, up, down)


def prepare_kernel(place, small, large, latent, rope_key, cosine_of, sine_of, query, packed, tall):
    _, _, x, core = where_in(place[0])
    half = ROPE // 2
    cosine = cosine_of[...]
    sine = sine_of[...]

    def turn(v):
        v = v.astype(jnp.float32)
        leading = v[0:half, :]
        trailing = v[half:, :]
        return jnp.concatenate(
            [leading * cosine - trailing * sine, trailing * cosine + leading * sine], axis=0
        )

    tall[...] = latent[...].astype(jnp.float32).T
    mine = tall[pl.ds(pl.multiple_of(64 * x + 32 * core, 32), 32), :]
    piece = jnp.concatenate([mine, turn(rope_key[...])], axis=0).astype(jnp.bfloat16)
    for k in range(packed.shape[0]):
        packed[k] = piece
    upright = jnp.concatenate(
        [
            large[0:HEAD_LARGE, :].astype(jnp.float32),
            small[0:HEAD_SMALL, :].astype(jnp.float32),
            turn(small[HEAD_SMALL:, :]) * SCALE_SMALL,
            turn(large[HEAD_LARGE:, :]) * SCALE_LARGE,
        ],
        axis=0,
    )
    query[...] = upright.T.astype(jnp.bfloat16)


def prepare(place, small, large, latent, rope_key, cosine, sine, n_z):
    rows = latent.shape[0]
    return pl.pallas_call(
        prepare_kernel,
        out_shape=(
            jax.ShapeDtypeStruct((rows, 256), jnp.bfloat16),
            jax.ShapeDtypeStruct((n_z, 32 + ROPE, rows), jnp.bfloat16),
        ),
        in_specs=[SMEM] + [VMEM] * 6,
        out_specs=(VMEM, VMEM),
        scratch_shapes=[pltpu.VMEM((256, rows), jnp.float32)],
        compiler_params=pltpu.CompilerParams(vmem_limit_bytes=4 * MIB),
        name="prepare",
    )(place, small, large, latent, rope_key, cosine, sine)


def join_kernel(place, *refs):
    *queries, out = refs
    n_y = len(queries)
    _, y, _, _ = where_in(place[0])
    for k, query in enumerate(queries):
        out[lax.rem(y - k + n_y, n_y)] = query[...]


def join(place, queries):
    return pl.pallas_call(
        join_kernel,
        out_shape=jax.ShapeDtypeStruct((len(queries), *queries[0].shape), jnp.bfloat16),
        in_specs=[SMEM] + [VMEM] * len(queries),
        out_specs=VMEM,
        compiler_params=pltpu.CompilerParams(vmem_limit_bytes=4 * MIB),
        name="join",
    )(place, *queries)


def absorb_kernel(place, query, key_up_s, key_up_l, out):
    n_y = query.shape[0]
    _, y, _, _ = where_in(place[0])
    row = lax.broadcasted_iota(jnp.int32, (128, 128), 0)
    lane = lax.broadcasted_iota(jnp.int32, (128, 128), 1)
    diagonal = jnp.where(row == lane, 1.0, 0.0)
    pick_lane = lax.broadcasted_iota(jnp.int32, (128, 96), 1)
    key_up_large = key_up_l[...].T
    for j in range(n_y):
        q = query[j]
        own = jnp.where(y == j, diagonal, 0.0)
        pick = jnp.where(pick_lane == j, 1.0, 0.0)
        heads = (
            (q[:, 0:128], q[:, 224:256], key_up_large, SCALE_LARGE),
            (q[:, 128:192], q[:, 192:224], key_up_s[...], SCALE_SMALL),
        )
        for h, (nope, rope, key_up, scale) in enumerate(heads):
            wide = jnp.dot(nope, key_up, preferred_element_type=jnp.float32)
            tail = jnp.concatenate([rope.astype(jnp.float32), pick], axis=1)
            whole = jnp.concatenate([wide * scale, tail, own], axis=1)
            out[j, h, :, :] = whole.astype(jnp.bfloat16)


def absorb(place, query, key_up_s, key_up_l):
    n_y, rows = query.shape[:2]
    return pl.pallas_call(
        absorb_kernel,
        out_shape=jax.ShapeDtypeStruct((n_y, 2, rows, 512), jnp.bfloat16),
        in_specs=[SMEM] + [VMEM] * 3,
        out_specs=VMEM,
        compiler_params=pltpu.CompilerParams(vmem_limit_bytes=8 * MIB),
        name="absorb",
    )(place, query, key_up_s, key_up_l)


def attention_kernel(place, query, mine, other, ropes, value_up_s, value_up_l, out, keys):
    z, y, _, c = where_in(place[0])
    n_x, n_z = mine.shape[0], mine.shape[1]
    n_y = query.shape[0]
    row = lax.broadcasted_iota(jnp.int32, (128, 128), 0)
    lane = lax.broadcasted_iota(jnp.int32, (128, 128), 1)
    for k in range(n_z):
        lanes = pl.ds(128 * k, 128)
        for x in range(n_x):
            here = pl.multiple_of(64 * x + 32 * c, 32)
            there = pl.multiple_of(64 * x + 32 * (1 - c), 32)
            keys[pl.ds(here, 32), lanes] = mine[x, k]
            keys[pl.ds(there, 32), lanes] = other[x, k]
        keys[256 : 256 + ROPE, lanes] = ropes[k, 32:, :]
        hidden_from = (k > z) | ((k == z) & (y > row))
        bias = jnp.where(hidden_from & (row < n_y), big_negative, 0.0)
        keys[288:384, lanes] = bias[0:96, :].astype(jnp.bfloat16)
        later = jnp.where((lane > row) & (k == z), big_negative, 0.0)
        keys[384:512, lanes] = later.astype(jnp.bfloat16)
    stat_lane = lax.broadcasted_iota(jnp.int32, (128, 64), 1)

    full = query[...].reshape(n_y * 256, query.shape[3])
    score = jnp.dot(full, keys[...], preferred_element_type=jnp.float32)
    tops = jnp.max(score, axis=1, keepdims=True)
    weight = jnp.exp(score - tops)
    totals = jnp.sum(weight, axis=1, keepdims=True)
    summed = lax.dot_general(
        weight.astype(jnp.bfloat16), keys[0:256, :], NT, preferred_element_type=jnp.float32
    )
    summed = (summed / totals).astype(jnp.bfloat16)
    for j in range(n_y):
        large = slice(256 * j, 256 * j + 128)
        small = slice(256 * j + 128, 256 * j + 256)
        value_l = jnp.dot(summed[large], value_up_l[...], preferred_element_type=jnp.float32)
        value_s = lax.dot_general(
            summed[small], value_up_s[...], NT, preferred_element_type=jnp.float32
        )
        stats = jnp.zeros((128, 64), jnp.float32)
        parts = [
            p for v in (tops[large], totals[large], tops[small], totals[small]) for p in three_parts(v)
        ]
        for i, part in enumerate(parts):
            stats = jnp.where(stat_lane == i, part, stats)
        whole = jnp.concatenate([value_l, jnp.concatenate([value_s, stats], axis=1)], axis=1)
        for core in range(2):
            picked = [whole[32 * x + 16 * core : 32 * x + 16 * core + 16] for x in range(n_x)]
            out[2 * j + core] = jnp.concatenate(picked, axis=0).astype(jnp.bfloat16)


def attention(place, query, mine, other, ropes, value_up_s, value_up_l):
    n_y, _, rows, depth = query.shape
    n_keys = 128 * mine.shape[1]
    return pl.pallas_call(
        attention_kernel,
        out_shape=jax.ShapeDtypeStruct((2 * n_y, rows // 2, 256), jnp.bfloat16),
        in_specs=[SMEM] + [VMEM] * 6,
        out_specs=VMEM,
        scratch_shapes=[pltpu.VMEM((depth, n_keys), jnp.bfloat16)],
        compiler_params=pltpu.CompilerParams(vmem_limit_bytes=36 * MIB),
        name="attend",
    )(place, query, mine, other, ropes, value_up_s, value_up_l)


def merge_kernel(place, parts, own_s, own_l, their_s, their_l, out):
    _, _, _, core = where_in(place[0])
    n_y = parts.shape[0] // 2

    def attended(column):
        pieces = [parts[2 * i + column].astype(jnp.float32) for i in range(n_y)]

        def merged(first, width, stat):
            def stat_of(piece, which):
                at = 192 + stat + 3 * which
                return (piece[:, at : at + 1] + piece[:, at + 1 : at + 2]) + piece[:, at + 2 : at + 3]

            tops = [stat_of(piece, 0) for piece in pieces]
            top = tops[0]
            for t in tops[1:]:
                top = jnp.maximum(top, t)
            shares = [stat_of(p, 1) * jnp.exp(t - top) for p, t in zip(pieces, tops)]
            total = sum(shares[1:], shares[0])
            acc = 0.0
            for piece, share in zip(pieces, shares):
                acc = acc + piece[:, first : first + width] * (share / total)
            return acc.astype(jnp.bfloat16)

        return merged(0, HEAD_LARGE, 0), merged(HEAD_LARGE, HEAD_SMALL, 6)

    total = None
    for column, small_w, large_w in ((core, own_s, own_l), (1 - core, their_s, their_l)):
        large, small = attended(column)
        term = jnp.dot(large, large_w[...], preferred_element_type=jnp.float32) + jnp.dot(
            small, small_w[...], preferred_element_type=jnp.float32
        )
        total = term if total is None else total + term
    out[...] = total.astype(jnp.bfloat16)


def merge(place, parts, own_s, own_l, their_s, their_l):
    return pl.pallas_call(
        merge_kernel,
        out_shape=jax.ShapeDtypeStruct((parts.shape[1], own_s.shape[1]), jnp.bfloat16),
        in_specs=[SMEM] + [VMEM] * 5,
        out_specs=VMEM,
        compiler_params=pltpu.CompilerParams(vmem_limit_bytes=8 * MIB),
        name="merge",
    )(place, parts, own_s, own_l, their_s, their_l)


def fetch_kernel(weights, out, arrived):
    copy = pltpu.make_async_copy(weights, out, arrived)
    copy.start()
    copy.wait()


def fetch(weights):
    return pl.pallas_call(
        fetch_kernel,
        out_shape=jax.ShapeDtypeStruct(weights.shape, weights.dtype),
        in_specs=[pl.BlockSpec(memory_space=pltpu.HBM)],
        out_specs=VMEM,
        scratch_shapes=[pltpu.SemaphoreType.DMA],
        compiler_params=pltpu.CompilerParams(vmem_limit_bytes=46 * MIB),
        name="fetch",
    )(weights)


def mixer_kernel(rows, weights, out):
    room = weights.shape[1] // 3
    both = jnp.dot(rows[...], weights[:, 0 : 2 * room], preferred_element_type=jnp.float32)
    gate = both[:, :room]
    hidden = (gate / (1.0 + jnp.exp(-gate)) * both[:, room:]).astype(jnp.bfloat16)
    part = lax.dot_general(hidden, weights[:, 2 * room :], NT, preferred_element_type=jnp.float32)
    out[...] = part.astype(out.dtype)


def mixer(rows, weights, dtype):
    return pl.pallas_call(
        mixer_kernel,
        out_shape=jax.ShapeDtypeStruct(rows.shape, dtype),
        in_specs=[VMEM] * 2,
        out_specs=VMEM,
        compiler_params=pltpu.CompilerParams(vmem_limit_bytes=16 * MIB),
    )(rows, weights)


def shards(
    residual,
    query_small,
    query_large,
    latent,
    rope_key,
    key_up_small,
    value_up_small,
    key_up_large,
    value_up_large,
    out_small,
    out_large,
    norm_gain,
    gate_weight,
    up_weight,
    down_weight,
):
    n_y = lax.axis_size(("yh", "yl"))
    z = lax.axis_index("z")
    y = lax.axis_index(("yh", "yl"))
    x = lax.axis_index("x")
    c = lax.axis_index("c")
    row_count = query_small.shape[0]
    rows, d = residual.shape
    place = (((z * n_y + y) * lax.axis_size("x") + x) * 2 + c).astype(jnp.int32).reshape(1)

    chunks = pack_weights(gate_weight, up_weight, down_weight, n_y)
    over_y = exchanged(chunks, ("yh", "yl"))
    weights = lax.all_gather(
        over_y.reshape(-1, over_y.shape[2]), "z", axis=0, tiled=True
    )

    their_small = partner(out_small)
    their_large = partner(out_large)

    positions = (z * n_y + y) * row_count + jnp.arange(row_count, dtype=jnp.int32)
    inverse = 1.0 / rope_base ** (jnp.arange(0, ROPE, 2, dtype=jnp.float32) / ROPE)
    angles = positions.astype(jnp.float32)[None, :] * inverse[:, None]
    query, packed = prepare(
        place,
        query_small.T,
        query_large.T,
        latent,
        rope_key.T,
        jnp.cos(angles),
        jnp.sin(angles),
        lax.axis_size("z"),
    )
    along_z = exchanged(packed, "z")
    queries = [query] + [
        lax.ppermute(query, ("yh", "yl"), [(i, (i + k) % n_y) for i in range(n_y)])
        for k in range(1, n_y)
    ]
    full = absorb(place, join(place, queries), key_up_small.T, key_up_large)
    mine = from_everyone(along_z[:, :32], "x")
    other = partner(mine)

    partial = attention(place, full, mine, other, along_z, value_up_small.T, value_up_large)
    parts = exchanged(partial, ("yh", "yl", "c"))
    mixed_part = merge(place, parts, out_small, out_large, their_small, their_large)
    tiles = exchanged(mixed_part.reshape(-1, rows, d), "x")
    mixed = jnp.sum(tiles.astype(jnp.float32), axis=0).astype(jnp.bfloat16)
    stream = (residual.astype(jnp.float32) + mixed.astype(jnp.float32)).astype(jnp.bfloat16)
    as_float = stream.astype(jnp.float32)
    normed = as_float * lax.rsqrt(jnp.mean(as_float * as_float, axis=-1, keepdims=True) + norm_eps)
    gain = norm_gain.astype(jnp.float32)
    normed = (normed * gain[None, :]).astype(jnp.bfloat16)

    here = from_everyone(normed, ("yl", "x")).reshape(-1, d)
    here, weights = lax.optimization_barrier((here, weights))
    there = partner(here)
    held = fetch(weights)
    part_there = mixer(there, held, jnp.bfloat16)
    sent = partner(part_there)
    part_here = mixer(here, held, jnp.float32)
    both = (part_here + sent.astype(jnp.float32)).astype(jnp.bfloat16)
    pieces = exchanged(both.reshape(-1, rows, d), ("yl", "x"))
    channel = jnp.sum(pieces.astype(jnp.float32), axis=0).astype(jnp.bfloat16)
    return (as_float + 0.5 * channel.astype(jnp.float32)).astype(jnp.bfloat16)


def solution(mesh):
    fine = Mesh(mesh.devices.reshape(-1, 2, 2, 4, 2), ("z", "yh", "yl", "x", "c"))
    sp = ("z", "yh", "yl")
    tp = ("x", "c")
    both = sp + tp
    placed = (
        P(both, None),
        P(sp, tp),
        P(sp, tp),
        P(sp, None),
        P(sp, None),
        P(None, tp),
        P(None, tp),
        P(None, tp),
        P(None, tp),
        P(tp, None),
        P(tp, None),
        P(),
        P(sp, tp),
        P(sp, tp),
        P(sp, tp),
    )
    return jax.shard_map(
        shards, mesh=fine, in_specs=placed, out_specs=P(both, None), check_vma=False
    )
```

```python
import jax
import jax.numpy as jnp
from jax import lax
from jax.experimental import pallas as pl
from jax.experimental.pallas import tpu as pltpu
from jax.sharding import Mesh
from jax.sharding import PartitionSpec as P


HEAD_SMALL = 64
HEAD_LARGE = 128
ROPE = 32
SCALE_SMALL = (HEAD_SMALL + ROPE) ** (-0.5)
SCALE_LARGE = (HEAD_LARGE + ROPE) ** (-0.5)

big_negative = -1e30
rope_base = 500000.0
norm_eps = 1e-06

NT = (((1,), (1,)), ((), ()))
MIB = 1024 * 1024
VMEM = pl.BlockSpec(memory_space=pltpu.VMEM)
SMEM = pl.BlockSpec(memory_space=pltpu.SMEM)


def where_in(place):
    core = lax.rem(place, 2)
    x = lax.rem(lax.div(place, 2), 4)
    y = lax.rem(lax.div(place, 8), 4)
    return lax.div(place, 32), y, x, core


def from_everyone(shard, axis):
    copies = jnp.broadcast_to(shard, (lax.axis_size(axis), *shard.shape))
    return lax.all_to_all(copies, axis, split_axis=0, concat_axis=0, tiled=True)


def exchanged(chunks, axis):
    return lax.all_to_all(chunks, axis, split_axis=0, concat_axis=0, tiled=True)


def partner(x):
    return lax.ppermute(x, "c", [(0, 1), (1, 0)])


def three_parts(v):
    high = v.astype(jnp.bfloat16).astype(jnp.float32)
    rest = v - high
    middle = rest.astype(jnp.bfloat16).astype(jnp.float32)
    low = (rest - middle).astype(jnp.bfloat16).astype(jnp.float32)
    return [high, middle, low]


def weights_kernel(gate, up, down, out):
    cut = gate.shape[1] // 2
    room = out.shape[2] // 3
    depth = gate.shape[0]
    blank = jnp.zeros((depth, room - cut), jnp.bfloat16)
    for k, w in enumerate((gate, up, down)):
        first = jnp.concatenate([w[:, 0:cut], blank], axis=1)
        second = jnp.concatenate([w[:, cut:], blank], axis=1)
        for i in range(out.shape[0] // 2):
            out[2 * i, :, room * k : room * (k + 1)] = first
            out[2 * i + 1, :, room * k : room * (k + 1)] = second


def pack_weights(gate, up, down, n_y):
    room = -(-(gate.shape[1] // 2) // 128) * 128
    return pl.pallas_call(
        weights_kernel,
        out_shape=jax.ShapeDtypeStruct((n_y, gate.shape[0], 3 * room), jnp.bfloat16),
        in_specs=[VMEM] * 3,
        out_specs=VMEM,
        name="pack_weights",
    )(gate, up, down)


def prepare_kernel(place, small, large, latent, rope_key, cosine_of, sine_of, query, packed, tall):
    _, _, x, core = where_in(place[0])
    half = ROPE // 2
    cosine = cosine_of[...]
    sine = sine_of[...]

    def turn(v):
        v = v.astype(jnp.float32)
        leading = v[0:half, :]
        trailing = v[half:, :]
        return jnp.concatenate(
            [leading * cosine - trailing * sine, trailing * cosine + leading * sine], axis=0
        )

    tall[...] = latent[...].astype(jnp.float32).T
    mine = tall[pl.ds(pl.multiple_of(64 * x + 32 * core, 32), 32), :]
    piece = jnp.concatenate([mine, turn(rope_key[...])], axis=0).astype(jnp.bfloat16)
    for k in range(packed.shape[0]):
        packed[k] = piece
    upright = jnp.concatenate(
        [
            large[0:HEAD_LARGE, :].astype(jnp.float32),
            small[0:HEAD_SMALL, :].astype(jnp.float32),
            turn(small[HEAD_SMALL:, :]) * SCALE_SMALL,
            turn(large[HEAD_LARGE:, :]) * SCALE_LARGE,
        ],
        axis=0,
    )
    query[...] = upright.T.astype(jnp.bfloat16)


def prepare(place, small, large, latent, rope_key, cosine, sine, n_z):
    rows = latent.shape[0]
    return pl.pallas_call(
        prepare_kernel,
        out_shape=(
            jax.ShapeDtypeStruct((rows, 256), jnp.bfloat16),
            jax.ShapeDtypeStruct((n_z, 32 + ROPE, rows), jnp.bfloat16),
        ),
        in_specs=[SMEM] + [VMEM] * 6,
        out_specs=(VMEM, VMEM),
        scratch_shapes=[pltpu.VMEM((256, rows), jnp.float32)],
        compiler_params=pltpu.CompilerParams(vmem_limit_bytes=4 * MIB),
        name="prepare",
    )(place, small, large, latent, rope_key, cosine, sine)


def join_kernel(place, *refs):
    *queries, out = refs
    n_y = len(queries)
    _, y, _, _ = where_in(place[0])
    for k, query in enumerate(queries):
        out[lax.rem(y - k + n_y, n_y)] = query[...]


def join(place, queries):
    return pl.pallas_call(
        join_kernel,
        out_shape=jax.ShapeDtypeStruct((len(queries), *queries[0].shape), jnp.bfloat16),
        in_specs=[SMEM] + [VMEM] * len(queries),
        out_specs=VMEM,
        compiler_params=pltpu.CompilerParams(vmem_limit_bytes=4 * MIB),
        name="join",
    )(place, *queries)


def absorb_kernel(place, query, key_up_s, key_up_l, out):
    n_y = query.shape[0]
    _, y, _, _ = where_in(place[0])
    row = lax.broadcasted_iota(jnp.int32, (128, 128), 0)
    lane = lax.broadcasted_iota(jnp.int32, (128, 128), 1)
    diagonal = jnp.where(row == lane, 1.0, 0.0)
    pick_lane = lax.broadcasted_iota(jnp.int32, (128, 96), 1)
    key_up_large = key_up_l[...].T
    for j in range(n_y):
        q = query[j]
        own = jnp.where(y == j, diagonal, 0.0)
        pick = jnp.where(pick_lane == j, 1.0, 0.0)
        heads = (
            (q[:, 0:128], q[:, 224:256], key_up_large, SCALE_LARGE),
            (q[:, 128:192], q[:, 192:224], key_up_s[...], SCALE_SMALL),
        )
        for h, (nope, rope, key_up, scale) in enumerate(heads):
            wide = jnp.dot(nope, key_up, preferred_element_type=jnp.float32)
            tail = jnp.concatenate([rope.astype(jnp.float32), pick], axis=1)
            whole = jnp.concatenate([wide * scale, tail, own], axis=1)
            out[j, h, :, :] = whole.astype(jnp.bfloat16)


def absorb(place, query, key_up_s, key_up_l):
    n_y, rows = query.shape[:2]
    return pl.pallas_call(
        absorb_kernel,
        out_shape=jax.ShapeDtypeStruct((n_y, 2, rows, 512), jnp.bfloat16),
        in_specs=[SMEM] + [VMEM] * 3,
        out_specs=VMEM,
        compiler_params=pltpu.CompilerParams(vmem_limit_bytes=8 * MIB),
        name="absorb",
    )(place, query, key_up_s, key_up_l)


def attention_kernel(place, query, mine, other, ropes, value_up_s, value_up_l, out, keys):
    z, y, _, c = where_in(place[0])
    n_x, n_z = mine.shape[0], mine.shape[1]
    n_y = query.shape[0]
    row = lax.broadcasted_iota(jnp.int32, (128, 128), 0)
    lane = lax.broadcasted_iota(jnp.int32, (128, 128), 1)
    for k in range(n_z):
        lanes = pl.ds(128 * k, 128)
        for x in range(n_x):
            here = pl.multiple_of(64 * x + 32 * c, 32)
            there = pl.multiple_of(64 * x + 32 * (1 - c), 32)
            keys[pl.ds(here, 32), lanes] = mine[x, k]
            keys[pl.ds(there, 32), lanes] = other[x, k]
        keys[256 : 256 + ROPE, lanes] = ropes[k, 32:, :]
        hidden_from = (k > z) | ((k == z) & (y > row))
        bias = jnp.where(hidden_from & (row < n_y), big_negative, 0.0)
        keys[288:384, lanes] = bias[0:96, :].astype(jnp.bfloat16)
        later = jnp.where((lane > row) & (k == z), big_negative, 0.0)
        keys[384:512, lanes] = later.astype(jnp.bfloat16)
    stat_lane = lax.broadcasted_iota(jnp.int32, (128, 64), 1)

    full = query[...].reshape(n_y * 256, query.shape[3])
    score = jnp.dot(full, keys[...], preferred_element_type=jnp.float32)
    tops = jnp.max(score, axis=1, keepdims=True)
    weight = jnp.exp(score - tops)
    totals = jnp.sum(weight, axis=1, keepdims=True)
    summed = lax.dot_general(
        weight.astype(jnp.bfloat16), keys[0:256, :], NT, preferred_element_type=jnp.float32
    )
    summed = (summed / totals).astype(jnp.bfloat16)
    for j in range(n_y):
        large = slice(256 * j, 256 * j + 128)
        small = slice(256 * j + 128, 256 * j + 256)
        value_l = jnp.dot(summed[large], value_up_l[...], preferred_element_type=jnp.float32)
        value_s = lax.dot_general(
            summed[small], value_up_s[...], NT, preferred_element_type=jnp.float32
        )
        stats = jnp.zeros((128, 64), jnp.float32)
        parts = [
            p for v in (tops[large], totals[large], tops[small], totals[small]) for p in three_parts(v)
        ]
        for i, part in enumerate(parts):
            stats = jnp.where(stat_lane == i, part, stats)
        whole = jnp.concatenate([value_l, jnp.concatenate([value_s, stats], axis=1)], axis=1)
        for core in range(2):
            picked = [whole[32 * x + 16 * core : 32 * x + 16 * core + 16] for x in range(n_x)]
            out[2 * j + core] = jnp.concatenate(picked, axis=0).astype(jnp.bfloat16)


def attention(place, query, mine, other, ropes, value_up_s, value_up_l):
    n_y, _, rows, depth = query.shape
    n_keys = 128 * mine.shape[1]
    return pl.pallas_call(
        attention_kernel,
        out_shape=jax.ShapeDtypeStruct((2 * n_y, rows // 2, 256), jnp.bfloat16),
        in_specs=[SMEM] + [VMEM] * 6,
        out_specs=VMEM,
        scratch_shapes=[pltpu.VMEM((depth, n_keys), jnp.bfloat16)],
        compiler_params=pltpu.CompilerParams(vmem_limit_bytes=36 * MIB),
        name="attend",
    )(place, query, mine, other, ropes, value_up_s, value_up_l)


def merge_kernel(place, parts, own_s, own_l, their_s, their_l, out):
    _, _, _, core = where_in(place[0])
    n_y = parts.shape[0] // 2

    def attended(column):
        pieces = [parts[2 * i + column].astype(jnp.float32) for i in range(n_y)]

        def merged(first, width, stat):
            def stat_of(piece, which):
                at = 192 + stat + 3 * which
                return (piece[:, at : at + 1] + piece[:, at + 1 : at + 2]) + piece[:, at + 2 : at + 3]

            tops = [stat_of(piece, 0) for piece in pieces]
            top = tops[0]
            for t in tops[1:]:
                top = jnp.maximum(top, t)
            shares = [stat_of(p, 1) * jnp.exp(t - top) for p, t in zip(pieces, tops)]
            total = sum(shares[1:], shares[0])
            acc = 0.0
            for piece, share in zip(pieces, shares):
                acc = acc + piece[:, first : first + width] * (share / total)
            return acc.astype(jnp.bfloat16)

        return merged(0, HEAD_LARGE, 0), merged(HEAD_LARGE, HEAD_SMALL, 6)

    total = None
    for column, small_w, large_w in ((core, own_s, own_l), (1 - core, their_s, their_l)):
        large, small = attended(column)
        term = jnp.dot(large, large_w[...], preferred_element_type=jnp.float32) + jnp.dot(
            small, small_w[...], preferred_element_type=jnp.float32
        )
        total = term if total is None else total + term
    out[...] = total.astype(jnp.bfloat16)


def merge(place, parts, own_s, own_l, their_s, their_l):
    return pl.pallas_call(
        merge_kernel,
        out_shape=jax.ShapeDtypeStruct((parts.shape[1], own_s.shape[1]), jnp.bfloat16),
        in_specs=[SMEM] + [VMEM] * 5,
        out_specs=VMEM,
        compiler_params=pltpu.CompilerParams(vmem_limit_bytes=8 * MIB),
        name="merge",
    )(place, parts, own_s, own_l, their_s, their_l)


def fetch_kernel(weights, out, arrived):
    pieces = arrived.shape[0]
    rows = weights.shape[0] // pieces
    copies = [
        pltpu.make_async_copy(
            weights.at[pl.ds(rows * i, rows), :], out.at[pl.ds(rows * i, rows), :], arrived.at[i]
        )
        for i in range(pieces)
    ]
    for copy in copies:
        copy.start()
    for copy in copies:
        copy.wait()


def fetch(weights):
    return pl.pallas_call(
        fetch_kernel,
        out_shape=jax.ShapeDtypeStruct(weights.shape, weights.dtype),
        in_specs=[pl.BlockSpec(memory_space=pltpu.HBM)],
        out_specs=VMEM,
        scratch_shapes=[pltpu.SemaphoreType.DMA((4,))],
        compiler_params=pltpu.CompilerParams(vmem_limit_bytes=46 * MIB),
        name="fetch",
    )(weights)


def mixer_kernel(rows, weights, out):
    room = weights.shape[1] // 3
    both = jnp.dot(rows[...], weights[:, 0 : 2 * room], preferred_element_type=jnp.float32)
    gate = both[:, :room]
    hidden = (gate / (1.0 + jnp.exp(-gate)) * both[:, room:]).astype(jnp.bfloat16)
    part = lax.dot_general(hidden, weights[:, 2 * room :], NT, preferred_element_type=jnp.float32)
    out[...] = part.astype(out.dtype)


def mixer(rows, weights, dtype):
    return pl.pallas_call(
        mixer_kernel,
        out_shape=jax.ShapeDtypeStruct(rows.shape, dtype),
        in_specs=[VMEM] * 2,
        out_specs=VMEM,
        compiler_params=pltpu.CompilerParams(vmem_limit_bytes=16 * MIB),
    )(rows, weights)


def shards(
    residual,
    query_small,
    query_large,
    latent,
    rope_key,
    key_up_small,
    value_up_small,
    key_up_large,
    value_up_large,
    out_small,
    out_large,
    norm_gain,
    gate_weight,
    up_weight,
    down_weight,
):
    n_y = lax.axis_size(("yh", "yl"))
    z = lax.axis_index("z")
    y = lax.axis_index(("yh", "yl"))
    x = lax.axis_index("x")
    c = lax.axis_index("c")
    row_count = query_small.shape[0]
    rows, d = residual.shape
    place = (((z * n_y + y) * lax.axis_size("x") + x) * 2 + c).astype(jnp.int32).reshape(1)

    chunks = pack_weights(gate_weight, up_weight, down_weight, n_y)
    over_y = exchanged(chunks, ("yh", "yl"))
    weights = lax.all_gather(
        over_y.reshape(-1, over_y.shape[2]), "z", axis=0, tiled=True
    )

    their_small = partner(out_small)
    their_large = partner(out_large)

    positions = (z * n_y + y) * row_count + jnp.arange(row_count, dtype=jnp.int32)
    inverse = 1.0 / rope_base ** (jnp.arange(0, ROPE, 2, dtype=jnp.float32) / ROPE)
    angles = positions.astype(jnp.float32)[None, :] * inverse[:, None]
    query, packed = prepare(
        place,
        query_small.T,
        query_large.T,
        latent,
        rope_key.T,
        jnp.cos(angles),
        jnp.sin(angles),
        lax.axis_size("z"),
    )
    along_z = exchanged(packed, "z")
    queries = [query] + [
        lax.ppermute(query, ("yh", "yl"), [(i, (i + k) % n_y) for i in range(n_y)])
        for k in range(1, n_y)
    ]
    full = absorb(place, join(place, queries), key_up_small.T, key_up_large)
    mine = from_everyone(along_z[:, :32], "x")
    other = partner(mine)

    partial = attention(place, full, mine, other, along_z, value_up_small.T, value_up_large)
    parts = exchanged(partial, ("yh", "yl", "c"))
    mixed_part = merge(place, parts, out_small, out_large, their_small, their_large)
    tiles = exchanged(mixed_part.reshape(-1, rows, d), "x")
    mixed = jnp.sum(tiles.astype(jnp.float32), axis=0).astype(jnp.bfloat16)
    stream = (residual.astype(jnp.float32) + mixed.astype(jnp.float32)).astype(jnp.bfloat16)
    as_float = stream.astype(jnp.float32)
    normed = as_float * lax.rsqrt(jnp.mean(as_float * as_float, axis=-1, keepdims=True) + norm_eps)
    gain = norm_gain.astype(jnp.float32)
    normed = (normed * gain[None, :]).astype(jnp.bfloat16)

    here = from_everyone(normed, ("yl", "x")).reshape(-1, d)
    here, weights = lax.optimization_barrier((here, weights))
    there = partner(here)
    held = fetch(weights)
    part_there = mixer(there, held, jnp.bfloat16)
    sent = partner(part_there)
    part_here = mixer(here, held, jnp.float32)
    both = (part_here + sent.astype(jnp.float32)).astype(jnp.bfloat16)
    pieces = exchanged(both.reshape(-1, rows, d), ("yl", "x"))
    channel = jnp.sum(pieces.astype(jnp.float32), axis=0).astype(jnp.bfloat16)
    return (as_float + 0.5 * channel.astype(jnp.float32)).astype(jnp.bfloat16)


def solution(mesh):
    fine = Mesh(mesh.devices.reshape(-1, 2, 2, 4, 2), ("z", "yh", "yl", "x", "c"))
    sp = ("z", "yh", "yl")
    tp = ("x", "c")
    both = sp + tp
    placed = (
        P(both, None),
        P(sp, tp),
        P(sp, tp),
        P(sp, None),
        P(sp, None),
        P(None, tp),
        P(None, tp),
        P(None, tp),
        P(None, tp),
        P(tp, None),
        P(tp, None),
        P(),
        P(sp, tp),
        P(sp, tp),
        P(sp, tp),
    )
    return jax.shard_map(
        shards, mesh=fine, in_specs=placed, out_specs=P(both, None), check_vma=False
    )
```
